32 devices in a mesh: sp: 8 (over z, x), dp: 4 (over y, core).
Axes of the slice: x: 2, y: 2, z: 4, core: 2. Of those that a mesh axis runs over, the one named last changes fastest.
Arguments:
- resid: bfloat16 [4, 2048, 2048], P('dp', 'sp'), may hold values from -4 to 4
- query: bfloat16 [4, 2048, 2048], P('dp', 'sp'), may hold values from -6 to 6
- keys: bfloat16 [4, 2048, 512], P('dp', 'sp'), may hold values from -6 to 6
- values: bfloat16 [4, 2048, 512], P('dp', 'sp'), may hold values from -6 to 6
- q_gain: float32 [128], replicated, may hold values from 0.7 to 5
- k_gain: float32 [128], replicated, may hold values from 0.7 to 5
- out_weight: bfloat16 [2048, 2048], P('dp'), may hold values from -0.5 to 0.5
- norm_gain: float32 [2048], replicated, may hold values from 0.1 to 1.9
- route_ids: int32 [4, 2048, 2], P('dp', 'sp'), may hold values from 0 to 31, all different within a row; in each aligned block of 256 rows (0 to 255, 256 to 511, ..., all dimensions but the last counted through in order) at most 24 rows name the same one
- route_weight: float32 [4, 2048, 2], P('dp', 'sp'), may hold values from 0.2 to 1
- expert_gate: bfloat16 [32, 2048, 1024], P(('sp', 'dp')), may hold values from -0.125 to 0.125
- expert_up: bfloat16 [32, 2048, 1024], P(('sp', 'dp')), may hold values from -0.125 to 0.125
- expert_down: bfloat16 [32, 1024, 2048], P(('sp', 'dp')), may hold values from -0.1875 to 0.1875
Outputs:
- layer_out: bfloat16 [4, 2048, 2048], P('dp', 'sp')
The draws below stay inside these ranges and needn't reach their ends.
Inputs may be any that keep to these rules, and one draw needn't show every extreme that they name: `route_ids`: each row names 2 different experts. In the rows of one device no expert is named more than 24 times, and in some devices some expert is named exactly 24 times.
All inputs are finite; a program needn't handle non-finite values.
Results may differ from the reference program's by a relative error of at most 0.0095.
The reference program's roundings to bfloat16 on the way count: a program that leaves them out, or rounds other values in their place, can miss the bound.
Values may be sent and summed in bfloat16 or wider, within the bound.
A program may use at most 128 MiB of HBM per device.

```python
import math
import jax
import jax.numpy as jnp
import numpy as np
from jax import lax

D = 2048
QH = 16
KVH = 4
HD = 128
FE = 1024
TOP = 2
GRID_W = 64
TOK_DEV = 256
LEN = 2048
SEQS = 4
EXPERTS = 32
CAP = 24
N_SP = 8
N_DP = 4


def drawn_keys(key):
    return jnp.clip(jax.random.normal(jax.random.fold_in(key, 31), (SEQS, LEN, KVH * HD), jnp.float32), -6.0, 6.0)


def draw_keys(key, part):
    return drawn_keys(key).astype(jnp.bfloat16)


def draw_query(key, part):
    base = jnp.clip(jax.random.normal(jax.random.fold_in(key, 32), (SEQS, LEN, QH * HD), jnp.float32), -6.0, 6.0)
    return base.astype(jnp.bfloat16)


def gain_draw(key, salt):
    return jax.random.uniform(jax.random.fold_in(key, salt), (HD,), jnp.float32, 0.7, 1.6)


def draw_q_gain(key, part):
    return gain_draw(key, 41)


def draw_k_gain(key, part):
    return gain_draw(key, 42)


def block_levels(key, shape, split, low, high):
    factor_of, own = 1.0, jax.random.fold_in(key, 6)
    for position, parts in split:
        heights = jnp.exp(jax.random.uniform(jax.random.fold_in(own, position), (parts,), jnp.float32, low / len(split), high / len(split)))
        factor_of = factor_of * jnp.repeat(heights, shape[position] // parts).reshape([-1 if axis == position else 1 for axis in range(len(shape))])
    return factor_of


def routed_block(rng, own, number, rows, count, top, limit, slope):
    order = jax.random.permutation(rng, count)
    packed, ordinary = shares(count, rows * top, limit, slope, True), shares(count, rows * top, limit, slope, False)
    places = jnp.arange(count)

    def named(sizes, turn):
        used = int((sizes > 0).sum())
        fixed = max(1, used // 4)
        moved = fixed + (places - fixed + turn * (used - fixed)) % max(1, count - fixed)
        return jnp.zeros((count,), jnp.int32).at[order[jnp.where(places < fixed, places, moved)]].set(jnp.asarray(sizes, jnp.int32))

    sizes = jnp.where(number % 4 == 0, named(packed, number // 4), named(ordinary, number - number // 4 - 1))
    mixed = jax.random.permutation(jax.random.fold_in(own, 3), count)
    giver, sink = mixed[0:count // 2 * 2:2], mixed[1:count // 2 * 2:2]
    room = jnp.minimum(sizes[giver] - 1, limit - sizes[sink]) // 2
    room = jnp.where((giver == order[0]) | (sink == order[0]) | (sizes[sink] == 0), 0, jnp.maximum(room, 0))
    moved = jax.random.randint(jax.random.fold_in(own, 4), (count // 2,), 0, 1 << 20) % (room + 1)
    sizes = sizes.at[giver].add(-moved).at[sink].add(moved)
    labels = jnp.searchsorted(jnp.cumsum(sizes), jnp.arange(rows * top), side="right").astype(jnp.int32)
    grid = labels.reshape(top, rows).T
    grid = grid[jax.random.permutation(jax.random.fold_in(own, 1), rows)]
    turn = jax.random.randint(jax.random.fold_in(own, 2), (rows, 1), 0, top)
    return jnp.take_along_axis(grid, (jnp.arange(top)[None, :] + turn) % top, axis=1)


def shares(amount, total, bound, lean, full):
    weights = [(1 << 20) // math.isqrt(rank ** lean) + 1 for rank in range(1, amount + 1)]
    largest = bound if full else min(bound, max(-(-total // amount), total * weights[0] // sum(weights)))
    least = 1 if total - largest >= amount - 1 else 0
    given, spare = [largest] + [least] * (amount - 1), total - largest - least * (amount - 1)
    while spare > 0:
        candidates = [i for i in range(1, amount) if given[i] < largest] or [i for i in range(1, amount) if given[i] < bound]
        whole, left = sum([weights[i] for i in candidates]), spare
        for i in candidates:
            extra = min(bound - given[i], max(1, left * weights[i] // whole), spare)
            given[i] = given[i] + extra
            spare = spare - extra
    return np.array(given)


def scatter_about(rng, dims, width, most, split=(), kind=jnp.bfloat16):
    array = jax.random.normal(rng, dims, jnp.float32) * width
    if len(split) > 0:
        array = block_levels(rng, dims, split, -0.22, 0.18) * array
    return jnp.clip(array, min=-most, max=most).astype(kind)


def setup_inputs(seed: int = 0) -> dict:
    seeds = jax.random.split(jax.random.key(seed), 14)
    resid = scatter_about(seeds[0], (SEQS, LEN, D), 0.5, 4.0, ((0, 4), (1, 8)))
    query = draw_query(jax.random.fold_in(seeds[13], 71), 0)
    keys = draw_keys(jax.random.fold_in(seeds[13], 71), 0)
    values = scatter_about(seeds[3], (SEQS, LEN, KVH * HD), 1.0, 6.0, ((0, 4), (1, 8)))
    q_gain = draw_q_gain(jax.random.fold_in(seeds[13], 71), 0)
    k_gain = draw_k_gain(jax.random.fold_in(seeds[13], 71), 0)
    out_weight = scatter_about(seeds[6], (QH * HD, D), HD ** -0.5, 0.5, ((0, 4),))
    norm_gain = jnp.clip(1.0 + 0.18 * jax.random.normal(seeds[7], (D,), jnp.float32), 0.1, 1.9)
    route_ids_keys = jax.random.split(jax.random.fold_in(seeds[8], 1), SEQS * LEN // TOK_DEV)
    route_ids_turns = jax.random.permutation(jax.random.fold_in(seeds[8], 3), SEQS * LEN // TOK_DEV)
    route_ids = jax.vmap(lambda own, number: routed_block(jax.random.fold_in(seeds[8], 2), own, number, TOK_DEV, EXPERTS, TOP, CAP, 2))(route_ids_keys, route_ids_turns).reshape((SEQS, LEN, TOP))
    route_weight = jnp.clip(0.2 + 0.8 * jax.random.uniform(seeds[9], (SEQS, LEN, TOP), jnp.float32) ** block_levels(seeds[9], (SEQS, LEN, TOP), ((0, 4), (1, 8)), -0.2, 0.2), 0.2, 1.0)
    expert_gate = scatter_about(seeds[10], (EXPERTS, D, FE), D ** -0.5, 0.125, ((0, 32),))
    expert_up = scatter_about(seeds[11], (EXPERTS, D, FE), D ** -0.5, 0.125, ((0, 32),))
    expert_down = scatter_about(seeds[12], (EXPERTS, FE, D), FE ** -0.5, 0.1875, ((0, 32),))
    return {"resid": resid, "query": query, "keys": keys, "values": values, "q_gain": q_gain, "k_gain": k_gain, "out_weight": out_weight, "norm_gain": norm_gain, "route_ids": route_ids, "route_weight": route_weight, "expert_gate": expert_gate, "expert_up": expert_up, "expert_down": expert_down}


EPSILON = 1e-06
THETA = 10000.0
LIMIT = 7.0
SLOPE = 1.702

def turn_half(matrix, places):
    half_width = matrix.shape[-1] // 2
    inverse = THETA ** (-jnp.arange(half_width, dtype=jnp.float32) / half_width)
    angles = places.astype(jnp.float32)[:, None] * inverse[None, :]
    cosine = jnp.cos(angles)[:, None, :]
    sine_part = jnp.sin(angles)[:, None, :]
    leading = matrix[..., :half_width]
    second = matrix[..., half_width:]
    return jnp.concatenate([leading * cosine - second * sine_part, second * cosine + leading * sine_part], axis=-1)

def prepare(projected_rows, gain_vector, head_count, places):
    matrix = projected_rows.astype(jnp.float32).reshape(projected_rows.shape[0], head_count, -1)
    matrix = matrix * lax.rsqrt(lax.optimization_barrier(jnp.mean(matrix * matrix, axis=-1, keepdims=True)) + EPSILON) * gain_vector
    middle = matrix.shape[-1] // 2
    turned = jnp.concatenate([turn_half(matrix[..., :middle], places // GRID_W), turn_half(matrix[..., middle:], places % GRID_W)], axis=-1)
    return turned.astype(jnp.bfloat16)

def attend(head_query, head_key, head_value):
    length, local_heads, head_dim = head_query.shape
    local_kv = head_key.shape[1]
    group_size = local_heads // local_kv
    block_rows = min(512, length)
    scaling = head_dim ** (-0.5)
    query_blocks = head_query.reshape(length // block_rows, block_rows, local_kv, group_size, head_dim)
    key_wide = head_key.astype(jnp.float32)
    value_wide = head_value.astype(jnp.float32)

    def one_block(query_block):
        scores = jnp.einsum('qkgd,skd->kgqs', query_block.astype(jnp.float32), key_wide) * scaling
        lifted = jnp.exp(scores - lax.optimization_barrier(jnp.max(scores, axis=-1, keepdims=True)))
        attn_weights = (lifted / lax.optimization_barrier(jnp.sum(lifted, axis=-1, keepdims=True))).astype(jnp.bfloat16)
        return jnp.einsum('kgqs,skd->qkgd', attn_weights.astype(jnp.float32), value_wide).astype(jnp.bfloat16)
    return lax.map(one_block, query_blocks).reshape(length, local_heads, head_dim)

def apply_expert(batch, gate_matrix, up_matrix, down_matrix):
    flat_rows = batch.reshape(-1, batch.shape[-1])
    gated = jnp.minimum(jnp.dot(flat_rows, gate_matrix, preferred_element_type=jnp.float32), LIMIT)
    linear = jnp.clip(jnp.dot(flat_rows, up_matrix, preferred_element_type=jnp.float32), -LIMIT, LIMIT)
    active = (gated * jax.nn.sigmoid(SLOPE * gated) * (linear + 1.0)).astype(jnp.bfloat16)
    return jnp.dot(active, down_matrix, preferred_element_type=jnp.float32).astype(jnp.bfloat16).reshape(batch.shape)

def block_tables(block_ids, block_weights):
    chosen = block_ids.reshape(-1)
    onehot = (chosen[:, None] == jnp.arange(EXPERTS, dtype=jnp.int32)[None, :]).astype(jnp.int32)
    earlier = lax.optimization_barrier(jnp.sum((jnp.cumsum(onehot, axis=0) - onehot) * onehot, axis=1))
    target = (chosen * CAP + earlier).astype(jnp.int32)
    sources = jnp.arange(TOK_DEV * TOP, dtype=jnp.int32) // TOP
    slot_table = jnp.full((EXPERTS * CAP,), -1, jnp.int32).at[target].set(sources)
    slot_weight = jnp.zeros((EXPERTS * CAP,), jnp.float32).at[target].set(block_weights.reshape(-1))
    return (slot_table, slot_weight)

def reference(resid, query, keys, values, q_gain, k_gain, out_weight, norm_gain, route_ids, route_weight, expert_gate, expert_up, expert_down):
    places = jnp.arange(LEN, dtype=jnp.int32)

    def one_sequence(operands):
        query_rows, key_rows, value_rows = operands
        query_turned = prepare(query_rows, q_gain, QH, places)
        key_turned = prepare(key_rows, k_gain, KVH, places)
        mixed = attend(query_turned, key_turned, value_rows.reshape(LEN, KVH, HD))
        return mixed.reshape(LEN, QH * HD)
    head_out = lax.map(one_sequence, (query, keys, values))
    projected = jnp.dot(head_out.reshape(SEQS * LEN, QH * HD), out_weight, preferred_element_type=jnp.float32)
    updated = (resid.reshape(SEQS * LEN, D).astype(jnp.float32) + projected).astype(jnp.bfloat16)
    widened = updated.astype(jnp.float32)
    normed = (widened * lax.rsqrt(lax.optimization_barrier(jnp.mean(widened * widened, axis=-1, keepdims=True)) + EPSILON) * norm_gain).astype(jnp.bfloat16)
    block_count = N_SP * N_DP
    slot_table, slot_weight = jax.vmap(block_tables)(route_ids.reshape(block_count, TOK_DEV, TOP), route_weight.reshape(block_count, TOK_DEV, TOP))
    slot_table = jnp.transpose(slot_table.reshape(block_count, EXPERTS, CAP), (1, 0, 2))
    slot_weight = jnp.transpose(slot_weight.reshape(block_count, EXPERTS, CAP), (1, 0, 2))
    block_start = (jnp.arange(block_count, dtype=jnp.int32) * TOK_DEV)[:, None]

    def one_expert(running, operands):
        gate_matrix, up_matrix, down_matrix, table_rows, weight_rows = operands
        valid = table_rows >= 0
        global_rows = jnp.where(valid, table_rows + block_start, 0).reshape(-1).astype(jnp.int32)
        answered = apply_expert(normed[global_rows], gate_matrix, up_matrix, down_matrix)
        scaled = answered.astype(jnp.float32) * jnp.where(valid, weight_rows, 0.0).reshape(-1)[:, None]
        return (running.at[global_rows].add(scaled), None)
    combined = lax.scan(one_expert, jnp.zeros((SEQS * LEN, D), jnp.float32), (expert_gate, expert_up, expert_down, slot_table, slot_weight))[0]
    return (widened + combined).astype(jnp.bfloat16).reshape(SEQS, LEN, D)
```

```python
import functools

import jax
import jax.numpy as jnp
from jax import lax
from jax.experimental import pallas as pl
from jax.experimental.pallas import tpu as pltpu
from jax.sharding import PartitionSpec as P

GRID_W = 64
EPSILON = 1e-06
THETA = 10000.0
LIMIT = 7.0
SLOPE = 1.702
LOG2E = 1.4426950408889634
MESH = pl.DeviceIdType.MESH
VMEM_BYTES = 64000000
CHUNKS = 4


def split_of(count, inner):
    return (count // inner, inner) if count % inner == 0 else (count, 1)


def turn_tables(places, head_dim):
    quarter = head_dim // 4
    inverse = THETA ** (-jnp.arange(quarter, dtype=jnp.float32) / quarter)
    row = (places // GRID_W).astype(jnp.float32)[:, None] * inverse[None, :]
    col = (places % GRID_W).astype(jnp.float32)[:, None] * inverse[None, :]
    cosine = jnp.concatenate([jnp.cos(row)] * 2 + [jnp.cos(col)] * 2, axis=-1)
    sine = jnp.concatenate(
        [-jnp.sin(row), jnp.sin(row), -jnp.sin(col), jnp.sin(col)], axis=-1
    )
    return cosine, sine


def attention_kernel(
    planes, lanes_x, outer_dp, inner_dp,
    q_ref, k_ref, v_ref, qg_ref, kg_ref, cos_ref, sin_ref, resid_ref, ng_ref, w_ref,
    upd_ref, normed_ref,
    kall, vall, wall, qt, acc, mx, ls, head_out,
    kx_s, kx_r, kz_s, kz_r, vz_s, vz_r, vx_s, vx_r, wy_s, wy_r, wc_s, wc_r, loc,
):
    Z, X, Y, C = planes, lanes_x, outer_dp, inner_dp
    rows, head_dim = cos_ref.shape
    q_heads = q_ref.shape[1] // head_dim
    kv_heads = k_ref.shape[1] // head_dim
    group = q_heads // kv_heads
    w_rows = w_ref.shape[0]
    sp, dp = lax.axis_index("sp"), lax.axis_index("dp")
    z, x = sp // X, sp % X
    y, c = dp // C, dp % C
    up_ok, down_ok = z + 1 < Z, z > 0

    barrier = pltpu.get_barrier_semaphore()

    def greet(device):
        pl.semaphore_signal(barrier, inc=1, device_id=device, device_id_type=MESH)

    for j in range(1, X):
        greet((z * X + (x + j) % X, dp))

    @pl.when(up_ok)
    def _():
        greet((sp + X, dp))

    @pl.when(down_ok)
    def _():
        greet((sp - X, dp))

    for j in range(1, Y):
        greet((sp, ((y + j) % Y) * C + c))
    for j in range(1, C):
        greet((sp, y * C + (c + j) % C))

    def krows(block):
        return pl.ds(pl.multiple_of(block * rows, rows), rows)

    def wrows(block):
        return pl.ds(pl.multiple_of(block * w_rows, w_rows), w_rows)

    v_own = pltpu.make_async_copy(v_ref, vall.at[krows(sp)], loc.at[0])
    v_own.start()
    w_own = pltpu.make_async_copy(w_ref, wall.at[wrows(dp)], loc.at[1])
    w_own.start()

    lane = lax.broadcasted_iota(jnp.int32, (rows, head_dim), 1)
    first = lane % (head_dim // 2) < head_dim // 4

    def turned(value, gain):
        value = value.astype(jnp.float32)
        value = value * lax.rsqrt(jnp.mean(value * value, axis=-1, keepdims=True) + EPSILON) * gain
        swapped = jnp.where(
            first,
            pltpu.roll(value, head_dim - head_dim // 4, 1),
            pltpu.roll(value, head_dim // 4, 1),
        )
        return (value * cos_ref[...] + swapped * sin_ref[...]).astype(jnp.bfloat16)

    for g in range(kv_heads):
        span = slice(g * head_dim, (g + 1) * head_dim)
        kall[krows(sp), span] = turned(k_ref[:, span], kg_ref[...])

    count = (X - 1) + (Y - 1) + (C - 1) + up_ok.astype(jnp.int32) + down_ok.astype(jnp.int32)
    v_own.wait()
    w_own.wait()
    pl.semaphore_wait(barrier, count)

    def remote(buf, sl, ssem, rsem, device):
        return pltpu.make_async_remote_copy(
            src_ref=buf.at[sl], dst_ref=buf.at[sl], send_sem=ssem, recv_sem=rsem,
            device_id=device, device_id_type=MESH,
        )

    def kx(j):
        return remote(kall, krows(sp), kx_s.at[j], kx_r.at[j], (z * X + (x + j) % X, dp))

    def kz(d, s, j):
        plane = z - s if d == 0 else z + s
        device = (sp + X if d == 0 else sp - X, dp)
        at = (d * (Z - 1) + s) * X + j
        return remote(kall, krows(plane * X + (x + X - j) % X), kz_s.at[at], kz_r.at[at], device)

    def vz(d, s):
        plane = z - s if d == 0 else z + s
        device = (sp + X if d == 0 else sp - X, dp)
        at = d * (Z - 1) + s
        return remote(vall, krows(plane * X + x), vz_s.at[at], vz_r.at[at], device)

    def vx(slot, plane, j):
        at = slot * X + j
        return remote(
            vall, krows(plane * X + x), vx_s.at[at], vx_r.at[at], (z * X + (x + j) % X, dp)
        )

    def sends(d, s):
        if d == 0:
            return jnp.logical_and(up_ok, z - s >= 0)
        return jnp.logical_and(down_ok, z + s < Z)

    def gets(d, s):
        return z - s - 1 >= 0 if d == 0 else z + s + 1 < Z

    def wy(j):
        return remote(wall, wrows(dp), wy_s.at[j], wy_r.at[j], (sp, ((y + j) % Y) * C + c))

    def wc(j, i):
        at = j * C + i
        return remote(
            wall, wrows(((y + Y - j) % Y) * C + c), wc_s.at[at], wc_r.at[at],
            (sp, y * C + (c + i) % C),
        )

    for j in range(1, X):
        kx(j).start()
    for d in range(2):
        @pl.when(sends(d, 0))
        def _(d=d):
            kz(d, 0, 0).start()
            vz(d, 0).start()
    for j in range(1, X):
        vx(0, z, j).start()
    for j in range(1, Y):
        wy(j).start()
    for i in range(1, C):
        wc(0, i).start()

    def prepare_queries(h, carry):
        at = pl.ds(pl.multiple_of(h * head_dim, head_dim), head_dim)
        qt[h] = turned(q_ref[:, at], qg_ref[...])
        return carry

    lax.fori_loop(0, q_heads // 4, prepare_queries, 0)
    for j in range(1, X):
        kx(j).wait_recv()
    for d in range(2):
        @pl.when(sends(d, 0))
        def _(d=d):
            for j in range(1, X):
                kz(d, 0, j).start()
    lax.fori_loop(q_heads // 4, q_heads, prepare_queries, 0)

    factor = head_dim ** (-0.5) * LOG2E
    keys_in = X * rows

    def attend(plane, fresh):
        at_rows = pl.ds(pl.multiple_of(plane * keys_in, keys_in), keys_in)

        def one_group(i, carry):
            span = pl.ds(pl.multiple_of(i * head_dim, head_dim), head_dim)
            for u in range(group):
                h = i * group + u
                scores = lax.dot_general(
                    qt[h], kall[at_rows, span], (((1,), (1,)), ((), ())),
                    preferred_element_type=jnp.float32,
                )
                top = jnp.max(scores, axis=-1, keepdims=True)
                if not fresh:
                    before = mx[h]
                    top = jnp.maximum(before[:, :1], top)
                lifted = jnp.exp2((scores - top) * factor)
                total = jnp.sum(lifted, axis=-1, keepdims=True)
                part = jnp.dot(
                    lifted.astype(jnp.bfloat16), vall[at_rows, span],
                    preferred_element_type=jnp.float32,
                )
                wide = jnp.broadcast_to(top, (rows, head_dim))
                wide_total = jnp.broadcast_to(total, (rows, head_dim))
                if fresh:
                    acc[h], ls[h] = part, wide_total
                else:
                    fade = jnp.exp2((before - wide) * factor)
                    acc[h] = acc[h] * fade + part
                    ls[h] = ls[h] * fade + wide_total
                mx[h] = wide
            return carry

        lax.fori_loop(0, kv_heads, one_group, 0)

    def wait_vx(slot, plane):
        for j in range(1, X):
            vx(slot, plane, j).wait_recv()

    def attend_step(s):
        def one(t, carry):
            plane = jnp.where(t == 0, z - s - 1, z + s + 1)

            @pl.when(jnp.logical_and(plane >= 0, plane < Z))
            def _():
                wait_vx(1 + s + t * (Z - 1), plane)
                attend(plane, False)
            return carry

        lax.fori_loop(0, 2, one, 0)

    for s in range(Z - 1):
        for d in range(2):
            @pl.when(gets(d, s))
            def _(d=d, s=s):
                plane = z - s - 1 if d == 0 else z + s + 1
                vz(d, s).wait_recv()
                for j in range(1, X):
                    vx(1 + s + d * (Z - 1), plane, j).start()
                if s + 1 < Z - 1:
                    @pl.when(sends(d, s + 1))
                    def _():
                        vz(d, s + 1).start()
                for j in range(X):
                    kz(d, s, j).wait_recv()
                    if s + 1 < Z - 1:
                        @pl.when(sends(d, s + 1))
                        def _(j=j):
                            kz(d, s + 1, j).start()
        if s == 0:
            wait_vx(0, z)
            attend(z, True)
        else:
            attend_step(s - 1)

    for j in range(1, Y):
        wy(j).wait_recv()
        for i in range(1, C):
            wc(j, i).start()
    if Z == 1:
        wait_vx(0, z)
        attend(z, True)
    else:
        attend_step(Z - 2)

    for h in range(q_heads):
        head_out[:, h * head_dim:(h + 1) * head_dim] = (acc[h] / ls[h]).astype(jnp.bfloat16)

    for j in range(Y):
        for i in range(1, C):
            wc(j, i).wait_recv()

    width = wall.shape[1]
    tile = min(256, width)

    def project(n, total):
        at = pl.ds(pl.multiple_of(n * tile, tile), tile)
        projected = jnp.dot(head_out[...], wall[:, at], preferred_element_type=jnp.float32)
        updated = (resid_ref[:, at].astype(jnp.float32) + projected).astype(jnp.bfloat16)
        upd_ref[:, at] = updated
        wide = updated.astype(jnp.float32)
        return total + jnp.sum(wide * wide, axis=-1, keepdims=True)

    square = lax.fori_loop(0, width // tile, project, jnp.zeros((rows, 1), jnp.float32))
    scale = lax.rsqrt(square / width + EPSILON)

    def normalize(n, carry):
        at = pl.ds(pl.multiple_of(n * tile, tile), tile)
        normed_ref[:, at] = (
            upd_ref[:, at].astype(jnp.float32) * scale * ng_ref[:, at]
        ).astype(jnp.bfloat16)
        return carry

    lax.fori_loop(0, width // tile, normalize, 0)

    for j in range(1, X):
        kx(j).wait_send()
        vx(0, z, j).wait_send()
    for d in range(2):
        for s in range(Z - 1):
            @pl.when(sends(d, s))
            def _(d=d, s=s):
                vz(d, s).wait_send()
                for j in range(X):
                    kz(d, s, j).wait_send()

            @pl.when(gets(d, s))
            def _(d=d, s=s):
                plane = z - s - 1 if d == 0 else z + s + 1
                for j in range(1, X):
                    vx(1 + s + d * (Z - 1), plane, j).wait_send()
    for j in range(1, Y):
        wy(j).wait_send()
    for j in range(Y):
        for i in range(1, C):
            wc(j, i).wait_send()


def attention(query, keys, values, q_gain, k_gain, cosine, sine, resid, norm_gain, out_weight):
    sp_count, dp_count = lax.axis_size("sp"), lax.axis_size("dp")
    planes = 4 if sp_count % 4 == 0 else 1
    lanes_x = sp_count // planes
    outer_dp, inner_dp = split_of(dp_count, 2)
    rows, head_dim = cosine.shape
    q_heads = query.shape[1] // head_dim
    width = resid.shape[1]
    dma = pltpu.SemaphoreType.DMA
    vmem = pl.BlockSpec(memory_space=pltpu.VMEM)
    hops = 2 * max(planes - 1, 1)
    full_kv = (sp_count * rows, keys.shape[1])
    return pl.pallas_call(
        functools.partial(attention_kernel, planes, lanes_x, outer_dp, inner_dp),
        name="gathered_attention",
        out_shape=(
            jax.ShapeDtypeStruct((rows, width), jnp.bfloat16),
            jax.ShapeDtypeStruct((rows, width), jnp.bfloat16),
        ),
        in_specs=[vmem, vmem, pl.BlockSpec(memory_space=pl.ANY)]
        + [vmem] * 6
        + [pl.BlockSpec(memory_space=pl.ANY)],
        out_specs=(vmem, vmem),
        scratch_shapes=[
            pltpu.VMEM(full_kv, jnp.bfloat16),
            pltpu.VMEM(full_kv, jnp.bfloat16),
            pltpu.VMEM((dp_count * out_weight.shape[0], width), jnp.bfloat16),
            pltpu.VMEM((q_heads, rows, head_dim), jnp.bfloat16),
            pltpu.VMEM((q_heads, rows, head_dim), jnp.float32),
            pltpu.VMEM((q_heads, rows, head_dim), jnp.float32),
            pltpu.VMEM((q_heads, rows, head_dim), jnp.float32),
            pltpu.VMEM((rows, q_heads * head_dim), jnp.bfloat16),
            dma((lanes_x,)), dma((lanes_x,)),
            dma((hops * lanes_x,)), dma((hops * lanes_x,)),
            dma((hops,)), dma((hops,)),
            dma(((hops + 1) * lanes_x,)), dma(((hops + 1) * lanes_x,)),
            dma((outer_dp,)), dma((outer_dp,)),
            dma((outer_dp * inner_dp,)), dma((outer_dp * inner_dp,)),
            dma((2,)),
        ],
        compiler_params=pltpu.CompilerParams(
            collective_id=0, has_side_effects=True, vmem_limit_bytes=VMEM_BYTES
        ),
    )(
        query, keys, values, q_gain[None], k_gain[None], cosine, sine, resid,
        norm_gain[None], out_weight,
    )


def experts_kernel(
    planes, lanes_x, slots,
    meta_ref, normed_ref, upd_ref, gate_hbm, up_hbm, down_hbm,
    out_ref,
    meta, raw, pk, epk, xb, rb, fr, fp, ptab, whi, wlo, tri, xs, act, acc, gate_w, up_w, down_w,
    meta_s, meta_r, zs, zr, es, er, rs, rr, fs, fa, loc,
):
    Z, X, K = planes, lanes_x, slots
    rows, width = normed_ref.shape
    DP = lax.axis_size("dp")
    EP = X * DP
    S = EP * K
    top = meta_ref.shape[0] // 2
    chunks = zr.shape[1]
    part = width // chunks
    hidden = gate_w.shape[1]
    sp, dp = lax.axis_index("sp"), lax.axis_index("dp")
    z, x = sp // X, sp % X
    p = x * DP + dp
    f32, bf16 = jnp.float32, jnp.bfloat16

    def cols(ck):
        return pl.ds(pl.multiple_of(ck * part, part), part)

    def peer(q):
        return (z * X + q // DP, q % DP)

    def loop(low, high, body):
        def step(i, carry):
            body(i)
            return carry
        lax.fori_loop(low, high, step, 0)

    def remote(src, dst, ssem, rsem, device):
        return pltpu.make_async_remote_copy(
            src_ref=src, dst_ref=dst, send_sem=ssem, recv_sem=rsem,
            device_id=device, device_id_type=MESH,
        )

    weights = [
        pltpu.make_async_copy(gate_hbm, gate_w, loc.at[0]),
        pltpu.make_async_copy(up_hbm, up_w, loc.at[1]),
        pltpu.make_async_copy(down_hbm, down_w, loc.at[2]),
    ]

    barrier = pltpu.get_barrier_semaphore()

    def greet(device):
        pl.semaphore_signal(barrier, inc=1, device_id=device, device_id_type=MESH)

    loop(1, EP, lambda j: greet(peer((p + j) % EP)))
    for j in range(1, Z):
        greet((((z + j) % Z) * X + x, dp))
    for copy in weights:
        copy.start()
    tri[...] = (
        lax.broadcasted_iota(jnp.int32, (rows, rows), 0)
        < lax.broadcasted_iota(jnp.int32, (rows, rows), 1)
    ).astype(f32).astype(bf16)
    pl.semaphore_wait(barrier, EP - 1 + Z - 1)

    def side(d):
        return (sp + X if d == 0 else sp - X, dp)

    def exists(d):
        return z + 1 < Z if d == 0 else z >= 1

    def at_end(d):
        return z == Z - 1 if d == 0 else z == 0

    def next_end(d):
        return z + 1 == Z - 1 if d == 0 else z - 1 == 0

    def end_of(d):
        return Z - 1 if d == 0 else 0

    def meta_copy(j):
        return remote(
            meta_ref, meta.at[z], meta_s.at[j], meta_r.at[z], (((z + j) % Z) * X + x, dp)
        )

    def own_raw(d, ck):
        return remote(
            normed_ref.at[:, cols(ck)], raw.at[z, :, cols(ck)],
            zs.at[z if d == 0 else Z, ck], zr.at[z, ck], side(d),
        )

    def raw_on(d, src, ck):
        return remote(
            raw.at[src, :, cols(ck)], raw.at[src, :, cols(ck)],
            zs.at[src, ck], zr.at[src, ck], side(d),
        )

    def packed_on(d, src, slot, ck):
        return remote(
            epk.at[slot, :, :, cols(ck)], pk.at[src, :, :, cols(ck)],
            zs.at[slot, ck], zr.at[src, ck], side(d),
        )

    def landed(buf, index, sem):
        view = buf.at[index]
        pltpu.make_async_copy(view, view, sem).wait()

    def spread(src, ck):
        pltpu.make_async_copy(
            pk.at[src, p, :, cols(ck)], xb.at[src, p, :, cols(ck)], er.at[src, ck]
        ).start()

        def one(j):
            q = (p + j) % EP
            remote(
                pk.at[src, q, :, cols(ck)], xb.at[src, p, :, cols(ck)],
                es.at[src, ck], er.at[src, ck], peer(q),
            ).start()

        loop(1, EP, one)

    def give_back(src, ck):
        pltpu.make_async_copy(
            xb.at[src, p, :, cols(ck)], rb.at[src, p, :, cols(ck)], rr.at[src, ck]
        ).start()

        def one(j):
            q = (p + j) % EP
            remote(
                xb.at[src, q, :, cols(ck)], rb.at[src, p, :, cols(ck)],
                rs.at[src, ck], rr.at[src, ck], peer(q),
            ).start()

        loop(1, EP, one)

    def build(src, plane, index):
        info = meta[src]
        lane_expert = lax.broadcasted_iota(jnp.int32, (EP, rows), 0).astype(f32) + (
            plane * EP
        ).astype(f32) if not isinstance(plane, int) else (
            lax.broadcasted_iota(jnp.int32, (EP, rows), 0).astype(f32) + float(plane * EP)
        )
        named = jnp.zeros((EP, rows), f32)
        scale = jnp.zeros((EP, rows), f32)
        for i in range(top):
            hit = info[i:i + 1] == lane_expert
            named = jnp.where(hit, 1.0, named)
            scale = jnp.where(hit, info[top + i:top + i + 1], scale)
        rank = jnp.dot(named.astype(bf16), tri[...], preferred_element_type=f32)
        rank = jnp.where(named > 0.0, rank, -1.0)
        place = lax.broadcasted_iota(jnp.int32, (K, rows), 0).astype(f32)
        ones, scaled = [], []
        for e in range(EP):
            one = jnp.where(rank[e:e + 1] == place, 1.0, 0.0)
            ones.append(one)
            scaled.append(one * scale[e:e + 1])
        ptab[index] = jnp.concatenate(ones, axis=0).astype(bf16)
        spare = whi.shape[2] - S
        if spare:
            scaled.append(jnp.zeros((spare, rows), f32))
        turned = jnp.concatenate(scaled, axis=0).T
        high = turned.astype(bf16)
        whi[index] = high
        wlo[index] = (turned - high.astype(f32)).astype(bf16)

    def pack(index, value):
        got = jnp.dot(ptab[index], value, preferred_element_type=f32)
        return got.reshape(EP, K, part).astype(bf16)

    def unpack(index, value):
        flat = value.reshape(S, part)
        return jnp.dot(whi[index, :, :S], flat, preferred_element_type=f32) + jnp.dot(
            wlo[index, :, :S], flat, preferred_element_type=f32
        )

    for j in range(1, Z):
        meta_copy(j).start()
    for d in range(2):
        @pl.when(jnp.logical_and(exists(d), jnp.logical_not(next_end(d))))
        def _(d=d):
            loop(0, chunks, lambda ck: own_raw(d, ck).start())
    meta[z] = meta_ref[...]
    for d in range(2):
        @pl.when(jnp.logical_and(exists(d), next_end(d)))
        def _(d=d):
            slot = z if d == 0 else Z
            build(z, end_of(d), Z + slot)

            def chunk(ck):
                epk[slot, :, :, cols(ck)] = pack(Z + slot, normed_ref[:, cols(ck)])
                packed_on(d, z, slot, ck).start()

            loop(0, chunks, chunk)
    build(z, z, z)

    def own_chunk(ck):
        pk[z, :, :, cols(ck)] = pack(z, normed_ref[:, cols(ck)])
        spread(z, ck)

    loop(0, chunks, own_chunk)

    def carry_on(d, src):
        meta_arrived = pltpu.make_async_copy(meta.at[src], meta.at[src], meta_r.at[src])
        meta_arrived.wait()

        @pl.when(at_end(d))
        def _():
            def chunk(ck):
                landed(pk, (src, slice(None), slice(None), cols(ck)), zr.at[src, ck])
                spread(src, ck)

            loop(0, chunks, chunk)

        @pl.when(jnp.logical_not(at_end(d)))
        def _():
            build(src, z, src)

            @pl.when(next_end(d))
            def _():
                build(src, end_of(d), Z + src)

            def chunk(ck):
                landed(raw, (src, slice(None), cols(ck)), zr.at[src, ck])

                @pl.when(jnp.logical_not(next_end(d)))
                def _():
                    raw_on(d, src, ck).start()

                @pl.when(next_end(d))
                def _():
                    epk[src, :, :, cols(ck)] = pack(Z + src, raw[src, :, cols(ck)])
                    packed_on(d, src, src, ck).start()

                pk[src, :, :, cols(ck)] = pack(src, raw[src, :, cols(ck)])
                spread(src, ck)

            loop(0, chunks, chunk)

    tile = min(256, hidden)

    def run_expert(src):
        def gather(ck):
            landed(xb, (src, slice(None), slice(None), cols(ck)), er.at[src, ck])
            xs[:, cols(ck)] = xb[src, :, :, cols(ck)].reshape(S, part)

        loop(0, chunks, gather)

        def inner(n):
            at = pl.ds(pl.multiple_of(n * tile, tile), tile)
            gated = jnp.minimum(
                jnp.dot(xs[...], gate_w[:, at], preferred_element_type=f32), LIMIT
            )
            linear = jnp.clip(
                jnp.dot(xs[...], up_w[:, at], preferred_element_type=f32), -LIMIT, LIMIT
            )
            act[:, at] = (gated * jax.nn.sigmoid(SLOPE * gated) * (linear + 1.0)).astype(bf16)

        loop(0, hidden // tile, inner)

        def outer(ck):
            result = jnp.dot(act[...], down_w[:, cols(ck)], preferred_element_type=f32)
            xb[src, :, :, cols(ck)] = result.reshape(EP, K, part).astype(bf16)
            give_back(src, ck)

        loop(0, chunks, outer)

    def far_slot(d, src):
        return src if d == 0 else jnp.where(z + 1 == src, Z, src)

    def back_packed(d, src, ck):
        return remote(
            rb.at[src, :, :, cols(ck)], fp.at[far_slot(d, src), :, :, cols(ck)],
            fs.at[src, ck], fa.at[far_slot(d, src), ck], side(1 - d),
        )

    def back_raw(d, src, ck):
        return remote(
            raw.at[src, :, cols(ck)], fr.at[far_slot(d, src), :, cols(ck)],
            fs.at[src, ck], fa.at[far_slot(d, src), ck], side(1 - d),
        )

    def add_far(d, slot, ck):
        @pl.when(next_end(d))
        def _():
            landed(fp, (slot, slice(None), slice(None), cols(ck)), fa.at[slot, ck])
            acc[...] += unpack(Z + slot, fp[slot, :, :, cols(ck)])

        @pl.when(jnp.logical_not(next_end(d)))
        def _():
            landed(fr, (slot, slice(None), cols(ck)), fa.at[slot, ck])
            acc[...] += fr[slot, :, cols(ck)].astype(f32)

    def returned(src, ck):
        landed(rb, (src, slice(None), slice(None), cols(ck)), rr.at[src, ck])

    def send_back(d, src):
        def chunk(ck):
            returned(src, ck)

            @pl.when(at_end(d))
            def _():
                back_packed(d, src, ck).start()

            @pl.when(jnp.logical_not(at_end(d)))
            def _():
                acc[...] = unpack(src, rb[src, :, :, cols(ck)])
                add_far(d, src, ck)

                @pl.when(jnp.logical_not(next_end(d)))
                def _():
                    raw_on(d, src, ck).wait_send()

                raw[src, :, cols(ck)] = acc[...].astype(bf16)
                back_raw(d, src, ck).start()

        loop(0, chunks, chunk)

    def wait_weights():
        for copy in weights:
            copy.wait()

    def stage(s):
        for d in range(2):
            src = z - s if d == 0 else z + s

            @pl.when(src >= 0 if d == 0 else src < Z)
            def _(d=d, src=src):
                carry_on(d, src)

        @pl.when(s == 1)
        def _():
            wait_weights()

        def expert(t):
            src = jnp.where(t == 0, z, jnp.where(t == 1, z - s, z + s))
            fits = jnp.logical_and(src >= 0, src < Z)

            @pl.when(jnp.logical_and(fits, jnp.logical_or(t > 0, s == 1)))
            def _():
                run_expert(src)

        loop(0, 3, expert)
        for d in range(2):
            src = Z - 1 - s if d == 0 else s + 0 * z

            @pl.when(src < z if d == 0 else src > z)
            def _(d=d, src=src):
                send_back(d, src)

    if Z > 1:
        loop(1, Z, stage)
    else:
        wait_weights()
        run_expert(z)

    def finish(ck):
        returned(z, ck)
        acc[...] = upd_ref[:, cols(ck)].astype(f32) + unpack(z, rb[z, :, :, cols(ck)])
        for d in range(2):
            @pl.when(exists(d))
            def _(d=d):
                add_far(d, z if d == 0 else Z, ck)
        out_ref[:, cols(ck)] = acc[...].astype(bf16)

    loop(0, chunks, finish)

    for j in range(1, Z):
        meta_copy(j).wait_send()

    def sent_all(ck):
        for d in range(2):
            @pl.when(jnp.logical_and(exists(d), jnp.logical_not(next_end(d))))
            def _(d=d):
                own_raw(d, ck).wait_send()

            @pl.when(jnp.logical_and(exists(d), next_end(d)))
            def _(d=d):
                packed_on(d, z, z if d == 0 else Z, ck).wait_send()

        def per_source(src):
            some = pl.ds(0, EP - 1)
            landed(pk, (src, some, slice(None), cols(ck)), es.at[src, ck])
            landed(xb, (src, some, slice(None), cols(ck)), rs.at[src, ck])
            for d in range(2):
                @pl.when(src < z if d == 0 else src > z)
                def _(d=d):
                    @pl.when(at_end(d))
                    def _():
                        back_packed(d, src, ck).wait_send()

                    @pl.when(jnp.logical_not(at_end(d)))
                    def _():
                        back_raw(d, src, ck).wait_send()

                        @pl.when(next_end(d))
                        def _():
                            packed_on(d, src, src, ck).wait_send()

        loop(0, Z, per_source)

    loop(0, chunks, sent_all)


def experts(route_ids, route_weight, normed, updated, gate_matrix, up_matrix, down_matrix):
    sp_count, dp_count = lax.axis_size("sp"), lax.axis_size("dp")
    planes = 4 if sp_count % 4 == 0 else 1
    lanes_x = sp_count // planes
    rows, width = normed.shape
    top = route_ids.shape[1]
    capacity = max(2, 3 * rows * top // (2 * sp_count * dp_count))
    slots = -(-capacity // 8) * 8
    group = lanes_x * dp_count
    padded = -(-group * slots // 128) * 128
    hidden = gate_matrix.shape[1]
    chunks = CHUNKS if width % (128 * CHUNKS) == 0 else 1
    meta = jnp.concatenate([route_ids.astype(jnp.float32), route_weight], axis=1).T
    dma = pltpu.SemaphoreType.DMA
    vmem = pl.BlockSpec(memory_space=pltpu.VMEM)
    hbm = pl.BlockSpec(memory_space=pl.ANY)
    bf16, f32 = jnp.bfloat16, jnp.float32
    return pl.pallas_call(
        functools.partial(experts_kernel, planes, lanes_x, slots),
        name="routed_experts",
        out_shape=jax.ShapeDtypeStruct((rows, width), bf16),
        in_specs=[vmem] * 3 + [hbm] * 3,
        out_specs=vmem,
        scratch_shapes=[
            pltpu.VMEM((planes, 2 * top, rows), f32),
            pltpu.VMEM((planes, rows, width), bf16),
            pltpu.VMEM((planes, group, slots, width), bf16),
            pltpu.VMEM((planes + 1, group, slots, width), bf16),
            pltpu.VMEM((planes, group, slots, width), bf16),
            pltpu.VMEM((planes, group, slots, width), bf16),
            pltpu.VMEM((planes + 1, rows, width), bf16),
            pltpu.VMEM((planes + 1, group, slots, width), bf16),
            pltpu.VMEM((2 * planes + 1, group * slots, rows), bf16),
            pltpu.VMEM((2 * planes + 1, rows, padded), bf16),
            pltpu.VMEM((2 * planes + 1, rows, padded), bf16),
            pltpu.VMEM((rows, rows), bf16),
            pltpu.VMEM((group * slots, width), bf16),
            pltpu.VMEM((group * slots, hidden), bf16),
            pltpu.VMEM((rows, width // chunks), f32),
            pltpu.VMEM(gate_matrix.shape, bf16),
            pltpu.VMEM(up_matrix.shape, bf16),
            pltpu.VMEM(down_matrix.shape, bf16),
            dma((planes,)), dma((planes,)),
            dma((planes + 1, chunks)), dma((planes, chunks)),
            dma((planes, chunks)), dma((planes, chunks)),
            dma((planes, chunks)), dma((planes, chunks)),
            dma((planes, chunks)), dma((planes + 1, chunks)),
            dma((3,)),
        ],
        compiler_params=pltpu.CompilerParams(
            collective_id=1, has_side_effects=True, vmem_limit_bytes=VMEM_BYTES
        ),
    )(meta, normed, updated, gate_matrix, up_matrix, down_matrix)


def per_device(
    resid,
    query,
    keys,
    values,
    q_gain,
    k_gain,
    out_weight,
    norm_gain,
    route_ids,
    route_weight,
    expert_gate,
    expert_up,
    expert_down,
):
    tok_rows = resid.shape[1]
    head_dim = q_gain.shape[0]
    places = lax.axis_index("sp") * tok_rows + jnp.arange(tok_rows, dtype=jnp.int32)
    cosine, sine = turn_tables(places, head_dim)
    updated, normed = attention(
        query[0], keys[0], values[0], q_gain, k_gain, cosine, sine, resid[0], norm_gain, out_weight
    )
    return experts(
        route_ids[0], route_weight[0], normed, updated,
        expert_gate[0], expert_up[0], expert_down[0],
    )[None]


def solution(mesh):
    placed = (
        P("dp", "sp", None),
        P("dp", "sp", None),
        P("dp", "sp", None),
        P("dp", "sp", None),
        P(),
        P(),
        P("dp", None),
        P(),
        P("dp", "sp", None),
        P("dp", "sp", None),
        P(("sp", "dp"), None, None),
        P(("sp", "dp"), None, None),
        P(("sp", "dp"), None, None),
    )
    return jax.shard_map(
        per_device, mesh=mesh, in_specs=placed, out_specs=P("dp", "sp", None), check_vma=False
    )
```

```python
import functools

import jax
import jax.numpy as jnp
from jax import lax
from jax.experimental import pallas as pl
from jax.experimental.pallas import tpu as pltpu
from jax.sharding import PartitionSpec as P

GRID_W = 64
EPSILON = 1e-06
THETA = 10000.0
LIMIT = 7.0
SLOPE = 1.702
LOG2E = 1.4426950408889634
MESH = pl.DeviceIdType.MESH
VMEM_BYTES = 64000000
CHUNKS = 4


def split_of(count, inner):
    return (count // inner, inner) if count % inner == 0 else (count, 1)


def turn_tables(places, head_dim):
    quarter = head_dim // 4
    inverse = THETA ** (-jnp.arange(quarter, dtype=jnp.float32) / quarter)
    row = (places // GRID_W).astype(jnp.float32)[:, None] * inverse[None, :]
    col = (places % GRID_W).astype(jnp.float32)[:, None] * inverse[None, :]
    cosine = jnp.concatenate([jnp.cos(row)] * 2 + [jnp.cos(col)] * 2, axis=-1)
    sine = jnp.concatenate(
        [-jnp.sin(row), jnp.sin(row), -jnp.sin(col), jnp.sin(col)], axis=-1
    )
    return cosine, sine


def attention_kernel(
    planes, lanes_x, outer_dp, inner_dp,
    q_ref, k_ref, v_ref, qg_ref, kg_ref, cos_ref, sin_ref, resid_ref, ng_ref, w_ref,
    upd_ref, normed_ref,
    kall, vall, wall, qt, acc, mx, ls, head_out,
    kx_s, kx_r, kz_s, kz_r, vz_s, vz_r, vx_s, vx_r, wy_s, wy_r, wc_s, wc_r, loc,
):
    Z, X, Y, C = planes, lanes_x, outer_dp, inner_dp
    rows, head_dim = cos_ref.shape
    q_heads = q_ref.shape[1] // head_dim
    kv_heads = k_ref.shape[1] // head_dim
    group = q_heads // kv_heads
    w_rows = w_ref.shape[0]
    sp, dp = lax.axis_index("sp"), lax.axis_index("dp")
    z, x = sp // X, sp % X
    y, c = dp // C, dp % C
    up_ok, down_ok = z + 1 < Z, z > 0

    barrier = pltpu.get_barrier_semaphore()

    def greet(device):
        pl.semaphore_signal(barrier, inc=1, device_id=device, device_id_type=MESH)

    for j in range(1, X):
        greet((z * X + (x + j) % X, dp))

    @pl.when(up_ok)
    def _():
        greet((sp + X, dp))

    @pl.when(down_ok)
    def _():
        greet((sp - X, dp))

    for j in range(1, Y):
        greet((sp, ((y + j) % Y) * C + c))
    for j in range(1, C):
        greet((sp, y * C + (c + j) % C))

    def krows(block):
        return pl.ds(pl.multiple_of(block * rows, rows), rows)

    def wrows(block):
        return pl.ds(pl.multiple_of(block * w_rows, w_rows), w_rows)

    v_own = pltpu.make_async_copy(v_ref, vall.at[krows(sp)], loc.at[0])
    v_own.start()
    w_own = pltpu.make_async_copy(w_ref, wall.at[wrows(dp)], loc.at[1])
    w_own.start()

    lane = lax.broadcasted_iota(jnp.int32, (rows, head_dim), 1)
    first = lane % (head_dim // 2) < head_dim // 4

    def turned(value, gain):
        value = value.astype(jnp.float32)
        value = value * lax.rsqrt(jnp.mean(value * value, axis=-1, keepdims=True) + EPSILON) * gain
        swapped = jnp.where(
            first,
            pltpu.roll(value, head_dim - head_dim // 4, 1),
            pltpu.roll(value, head_dim // 4, 1),
        )
        return (value * cos_ref[...] + swapped * sin_ref[...]).astype(jnp.bfloat16)

    for g in range(kv_heads):
        span = slice(g * head_dim, (g + 1) * head_dim)
        kall[krows(sp), span] = turned(k_ref[:, span], kg_ref[...])

    count = (X - 1) + (Y - 1) + (C - 1) + up_ok.astype(jnp.int32) + down_ok.astype(jnp.int32)
    v_own.wait()
    w_own.wait()
    pl.semaphore_wait(barrier, count)

    def remote(buf, sl, ssem, rsem, device):
        return pltpu.make_async_remote_copy(
            src_ref=buf.at[sl], dst_ref=buf.at[sl], send_sem=ssem, recv_sem=rsem,
            device_id=device, device_id_type=MESH,
        )

    def kx(j):
        return remote(kall, krows(sp), kx_s.at[j], kx_r.at[j], (z * X + (x + j) % X, dp))

    def kz(d, s, j):
        plane = z - s if d == 0 else z + s
        device = (sp + X if d == 0 else sp - X, dp)
        at = (d * (Z - 1) + s) * X + j
        return remote(kall, krows(plane * X + (x + X - j) % X), kz_s.at[at], kz_r.at[at], device)

    def vz(d, s):
        plane = z - s if d == 0 else z + s
        device = (sp + X if d == 0 else sp - X, dp)
        at = d * (Z - 1) + s
        return remote(vall, krows(plane * X + x), vz_s.at[at], vz_r.at[at], device)

    def vx(slot, plane, j):
        at = slot * X + j
        return remote(
            vall, krows(plane * X + x), vx_s.at[at], vx_r.at[at], (z * X + (x + j) % X, dp)
        )

    def sends(d, s):
        if d == 0:
            return jnp.logical_and(up_ok, z - s >= 0)
        return jnp.logical_and(down_ok, z + s < Z)

    def gets(d, s):
        return z - s - 1 >= 0 if d == 0 else z + s + 1 < Z

    def wy(j):
        return remote(wall, wrows(dp), wy_s.at[j], wy_r.at[j], (sp, ((y + j) % Y) * C + c))

    def wc(j, i):
        at = j * C + i
        return remote(
            wall, wrows(((y + Y - j) % Y) * C + c), wc_s.at[at], wc_r.at[at],
            (sp, y * C + (c + i) % C),
        )

    for j in range(1, X):
        kx(j).start()
    for d in range(2):
        @pl.when(sends(d, 0))
        def _(d=d):
            kz(d, 0, 0).start()
            vz(d, 0).start()
    for j in range(1, X):
        vx(0, z, j).start()
    for j in range(1, Y):
        wy(j).start()
    for i in range(1, C):
        wc(0, i).start()

    def prepare_queries(h, carry):
        at = pl.ds(pl.multiple_of(h * head_dim, head_dim), head_dim)
        qt[h] = turned(q_ref[:, at], qg_ref[...])
        return carry

    lax.fori_loop(0, q_heads // 4, prepare_queries, 0)
    for j in range(1, X):
        kx(j).wait_recv()
    for d in range(2):
        @pl.when(sends(d, 0))
        def _(d=d):
            for j in range(1, X):
                kz(d, 0, j).start()
    lax.fori_loop(q_heads // 4, q_heads, prepare_queries, 0)

    factor = head_dim ** (-0.5) * LOG2E
    keys_in = X * rows

    def attend(plane, fresh):
        at_rows = pl.ds(pl.multiple_of(plane * keys_in, keys_in), keys_in)

        def one_group(i, carry):
            span = pl.ds(pl.multiple_of(i * head_dim, head_dim), head_dim)
            for u in range(group):
                h = i * group + u
                scores = lax.dot_general(
                    qt[h], kall[at_rows, span], (((1,), (1,)), ((), ())),
                    preferred_element_type=jnp.float32,
                )
                top = jnp.max(scores, axis=-1, keepdims=True)
                if not fresh:
                    before = mx[h]
                    top = jnp.maximum(before[:, :1], top)
                lifted = jnp.exp2((scores - top) * factor)
                total = jnp.sum(lifted, axis=-1, keepdims=True)
                part = jnp.dot(
                    lifted.astype(jnp.bfloat16), vall[at_rows, span],
                    preferred_element_type=jnp.float32,
                )
                wide = jnp.broadcast_to(top, (rows, head_dim))
                wide_total = jnp.broadcast_to(total, (rows, head_dim))
                if fresh:
                    acc[h], ls[h] = part, wide_total
                else:
                    fade = jnp.exp2((before - wide) * factor)
                    acc[h] = acc[h] * fade + part
                    ls[h] = ls[h] * fade + wide_total
                mx[h] = wide
            return carry

        lax.fori_loop(0, kv_heads, one_group, 0)

    def wait_vx(slot, plane):
        for j in range(1, X):
            vx(slot, plane, j).wait_recv()

    def attend_step(s):
        def one(t, carry):
            plane = jnp.where(t == 0, z - s - 1, z + s + 1)

            @pl.when(jnp.logical_and(plane >= 0, plane < Z))
            def _():
                wait_vx(1 + s + t * (Z - 1), plane)
                attend(plane, False)
            return carry

        lax.fori_loop(0, 2, one, 0)

    for s in range(Z - 1):
        for d in range(2):
            @pl.when(gets(d, s))
            def _(d=d, s=s):
                plane = z - s - 1 if d == 0 else z + s + 1
                vz(d, s).wait_recv()
                for j in range(1, X):
                    vx(1 + s + d * (Z - 1), plane, j).start()
                if s + 1 < Z - 1:
                    @pl.when(sends(d, s + 1))
                    def _():
                        vz(d, s + 1).start()
                for j in range(X):
                    kz(d, s, j).wait_recv()
                    if s + 1 < Z - 1:
                        @pl.when(sends(d, s + 1))
                        def _(j=j):
                            kz(d, s + 1, j).start()
        if s == 0:
            wait_vx(0, z)
            attend(z, True)
        else:
            attend_step(s - 1)

    for j in range(1, Y):
        wy(j).wait_recv()
        for i in range(1, C):
            wc(j, i).start()
    if Z == 1:
        wait_vx(0, z)
        attend(z, True)
    else:
        attend_step(Z - 2)

    for h in range(q_heads):
        head_out[:, h * head_dim:(h + 1) * head_dim] = (acc[h] / ls[h]).astype(jnp.bfloat16)

    for j in range(Y):
        for i in range(1, C):
            wc(j, i).wait_recv()

    width = wall.shape[1]
    tile = min(256, width)

    def project(n, total):
        at = pl.ds(pl.multiple_of(n * tile, tile), tile)
        projected = jnp.dot(head_out[...], wall[:, at], preferred_element_type=jnp.float32)
        updated = (resid_ref[:, at].astype(jnp.float32) + projected).astype(jnp.bfloat16)
        upd_ref[:, at] = updated
        wide = updated.astype(jnp.float32)
        return total + jnp.sum(wide * wide, axis=-1, keepdims=True)

    square = lax.fori_loop(0, width // tile, project, jnp.zeros((rows, 1), jnp.float32))
    scale = lax.rsqrt(square / width + EPSILON)

    def normalize(n, carry):
        at = pl.ds(pl.multiple_of(n * tile, tile), tile)
        normed_ref[:, at] = (
            upd_ref[:, at].astype(jnp.float32) * scale * ng_ref[:, at]
        ).astype(jnp.bfloat16)
        return carry

    lax.fori_loop(0, width // tile, normalize, 0)

    for j in range(1, X):
        kx(j).wait_send()
        vx(0, z, j).wait_send()
    for d in range(2):
        for s in range(Z - 1):
            @pl.when(sends(d, s))
            def _(d=d, s=s):
                vz(d, s).wait_send()
                for j in range(X):
                    kz(d, s, j).wait_send()

            @pl.when(gets(d, s))
            def _(d=d, s=s):
                plane = z - s - 1 if d == 0 else z + s + 1
                for j in range(1, X):
                    vx(1 + s + d * (Z - 1), plane, j).wait_send()
    for j in range(1, Y):
        wy(j).wait_send()
    for j in range(Y):
        for i in range(1, C):
            wc(j, i).wait_send()


def attention(query, keys, values, q_gain, k_gain, cosine, sine, resid, norm_gain, out_weight):
    sp_count, dp_count = lax.axis_size("sp"), lax.axis_size("dp")
    planes = 4 if sp_count % 4 == 0 else 1
    lanes_x = sp_count // planes
    outer_dp, inner_dp = split_of(dp_count, 2)
    rows, head_dim = cosine.shape
    q_heads = query.shape[1] // head_dim
    width = resid.shape[1]
    dma = pltpu.SemaphoreType.DMA
    vmem = pl.BlockSpec(memory_space=pltpu.VMEM)
    hops = 2 * max(planes - 1, 1)
    full_kv = (sp_count * rows, keys.shape[1])
    return pl.pallas_call(
        functools.partial(attention_kernel, planes, lanes_x, outer_dp, inner_dp),
        name="gathered_attention",
        out_shape=(
            jax.ShapeDtypeStruct((rows, width), jnp.bfloat16),
            jax.ShapeDtypeStruct((rows, width), jnp.bfloat16),
        ),
        in_specs=[vmem, vmem, pl.BlockSpec(memory_space=pl.ANY)]
        + [vmem] * 6
        + [pl.BlockSpec(memory_space=pl.ANY)],
        out_specs=(vmem, vmem),
        scratch_shapes=[
            pltpu.VMEM(full_kv, jnp.bfloat16),
            pltpu.VMEM(full_kv, jnp.bfloat16),
            pltpu.VMEM((dp_count * out_weight.shape[0], width), jnp.bfloat16),
            pltpu.VMEM((q_heads, rows, head_dim), jnp.bfloat16),
            pltpu.VMEM((q_heads, rows, head_dim), jnp.float32),
            pltpu.VMEM((q_heads, rows, head_dim), jnp.float32),
            pltpu.VMEM((q_heads, rows, head_dim), jnp.float32),
            pltpu.VMEM((rows, q_heads * head_dim), jnp.bfloat16),
            dma((lanes_x,)), dma((lanes_x,)),
            dma((hops * lanes_x,)), dma((hops * lanes_x,)),
            dma((hops,)), dma((hops,)),
            dma(((hops + 1) * lanes_x,)), dma(((hops + 1) * lanes_x,)),
            dma((outer_dp,)), dma((outer_dp,)),
            dma((outer_dp * inner_dp,)), dma((outer_dp * inner_dp,)),
            dma((2,)),
        ],
        compiler_params=pltpu.CompilerParams(
            collective_id=0, has_side_effects=True, vmem_limit_bytes=VMEM_BYTES
        ),
    )(
        query, keys, values, q_gain[None], k_gain[None], cosine, sine, resid,
        norm_gain[None], out_weight,
    )


def experts_kernel(
    planes, lanes_x, slots,
    meta_ref, normed_ref, upd_ref, gate_hbm, up_hbm, down_hbm,
    out_ref,
    meta, raw, pk, epk, xb, rb, fr, fp, ptab, whi, wlo, tri, xs, act, acc, gate_w, up_w, down_w,
    meta_s, meta_r, zs, zr, es, er, rs, rr, fs, fa, loc,
):
    Z, X, K = planes, lanes_x, slots
    rows, width = normed_ref.shape
    DP = lax.axis_size("dp")
    EP = X * DP
    S = EP * K
    top = meta_ref.shape[0] // 2
    chunks = zr.shape[1]
    part = width // chunks
    hidden = gate_w.shape[1]
    sp, dp = lax.axis_index("sp"), lax.axis_index("dp")
    z, x = sp // X, sp % X
    p = x * DP + dp
    f32, bf16 = jnp.float32, jnp.bfloat16

    def cols(ck):
        return pl.ds(pl.multiple_of(ck * part, part), part)

    def peer(q):
        return (z * X + q // DP, q % DP)

    def loop(low, high, body):
        def step(i, carry):
            body(i)
            return carry
        lax.fori_loop(low, high, step, 0)

    def remote(src, dst, ssem, rsem, device):
        return pltpu.make_async_remote_copy(
            src_ref=src, dst_ref=dst, send_sem=ssem, recv_sem=rsem,
            device_id=device, device_id_type=MESH,
        )

    weights = [
        pltpu.make_async_copy(gate_hbm, gate_w, loc.at[0]),
        pltpu.make_async_copy(up_hbm, up_w, loc.at[1]),
        pltpu.make_async_copy(down_hbm, down_w, loc.at[2]),
    ]

    barrier = pltpu.get_barrier_semaphore()

    def greet(device):
        pl.semaphore_signal(barrier, inc=1, device_id=device, device_id_type=MESH)

    loop(1, EP, lambda j: greet(peer((p + j) % EP)))
    for j in range(1, Z):
        greet((((z + j) % Z) * X + x, dp))
    for copy in weights:
        copy.start()
    tri[...] = (
        lax.broadcasted_iota(jnp.int32, (rows, rows), 0)
        < lax.broadcasted_iota(jnp.int32, (rows, rows), 1)
    ).astype(f32).astype(bf16)
    pl.semaphore_wait(barrier, EP - 1 + Z - 1)

    def toward(d):
        return 1 - 2 * d

    def side(d):
        return (sp + X * toward(d), dp)

    def end_of(d):
        return (Z - 1) * (1 - d)

    def exists(d):
        return jnp.logical_and(z + toward(d) >= 0, z + toward(d) < Z)

    def at_end(d):
        return z == end_of(d)

    def next_end(d):
        return z + toward(d) == end_of(d)

    def own_slot(d):
        return z + d * (Z - z)

    def meta_copy(j):
        return remote(
            meta_ref, meta.at[z], meta_s.at[j], meta_r.at[z], (((z + j) % Z) * X + x, dp)
        )

    def own_raw(d, ck):
        return remote(
            normed_ref.at[:, cols(ck)], raw.at[z, :, cols(ck)],
            zs.at[own_slot(d), ck], zr.at[z, ck], side(d),
        )

    def raw_on(d, src, ck):
        return remote(
            raw.at[src, :, cols(ck)], raw.at[src, :, cols(ck)],
            zs.at[src, ck], zr.at[src, ck], side(d),
        )

    def packed_on(d, src, slot, ck):
        return remote(
            epk.at[slot, :, :, cols(ck)], pk.at[src, :, :, cols(ck)],
            zs.at[slot, ck], zr.at[src, ck], side(d),
        )

    def landed(buf, index, sem):
        view = buf.at[index]
        pltpu.make_async_copy(view, view, sem).wait()

    def spread(src, ck):
        pltpu.make_async_copy(
            pk.at[src, p, :, cols(ck)], xb.at[src, p, :, cols(ck)], er.at[src, ck]
        ).start()

        def one(j):
            q = (p + j) % EP
            remote(
                pk.at[src, q, :, cols(ck)], xb.at[src, p, :, cols(ck)],
                es.at[src, ck], er.at[src, ck], peer(q),
            ).start()

        loop(1, EP, one)

    def give_back(src, ck):
        pltpu.make_async_copy(
            xb.at[src, p, :, cols(ck)], rb.at[src, p, :, cols(ck)], rr.at[src, ck]
        ).start()

        def one(j):
            q = (p + j) % EP
            remote(
                xb.at[src, q, :, cols(ck)], rb.at[src, p, :, cols(ck)],
                rs.at[src, ck], rr.at[src, ck], peer(q),
            ).start()

        loop(1, EP, one)

    def build(src, plane, index):
        info = meta[src]
        lane_expert = (
            lax.broadcasted_iota(jnp.int32, (EP, rows), 0) + plane * EP
        ).astype(f32)
        named = jnp.zeros((EP, rows), f32)
        scale = jnp.zeros((EP, rows), f32)
        for i in range(top):
            hit = info[i:i + 1] == lane_expert
            named = jnp.where(hit, 1.0, named)
            scale = jnp.where(hit, info[top + i:top + i + 1], scale)
        rank = jnp.dot(named.astype(bf16), tri[...], preferred_element_type=f32)
        rank = jnp.where(named > 0.0, rank, -1.0)
        place = lax.broadcasted_iota(jnp.int32, (K, rows), 0).astype(f32)
        ones, scaled = [], []
        for e in range(EP):
            one = jnp.where(rank[e:e + 1] == place, 1.0, 0.0)
            ones.append(one)
            scaled.append(one * scale[e:e + 1])
        ptab[index] = jnp.concatenate(ones, axis=0).astype(bf16)
        spare = whi.shape[2] - S
        if spare:
            scaled.append(jnp.zeros((spare, rows), f32))
        turned = jnp.concatenate(scaled, axis=0).T
        high = turned.astype(bf16)
        whi[index] = high
        wlo[index] = (turned - high.astype(f32)).astype(bf16)

    def pack(index, value):
        got = jnp.dot(ptab[index], value, preferred_element_type=f32)
        return got.reshape(EP, K, part).astype(bf16)

    def unpack(index, value):
        flat = value.reshape(S, part)
        return jnp.dot(whi[index, :, :S], flat, preferred_element_type=f32) + jnp.dot(
            wlo[index, :, :S], flat, preferred_element_type=f32
        )

    for j in range(1, Z):
        meta_copy(j).start()

    def own_raw_start(d):
        @pl.when(jnp.logical_and(exists(d), jnp.logical_not(next_end(d))))
        def _():
            loop(0, chunks, lambda ck: own_raw(d, ck).start())

    loop(0, 2, own_raw_start)
    meta[z] = meta_ref[...]

    def own_packed(d, low, high):
        @pl.when(jnp.logical_and(exists(d), next_end(d)))
        def _():
            slot = own_slot(d)

            def chunk(ck):
                epk[slot, :, :, cols(ck)] = pack(Z + slot, normed_ref[:, cols(ck)])
                packed_on(d, z, slot, ck).start()

            loop(low, high, chunk)

    def own_packed_start(d):
        @pl.when(jnp.logical_and(exists(d), next_end(d)))
        def _():
            build(z, end_of(d), Z + own_slot(d))

        own_packed(d, 0, early)

    early = -(-chunks // 2)
    last = chunks - 1
    is_end = jnp.logical_or(z == 0, z == Z - 1)
    loop(0, 2, own_packed_start)
    build(z, z, z)

    def own_chunk(ck):
        pk[z, :, :, cols(ck)] = pack(z, normed_ref[:, cols(ck)])
        spread(z, ck)

    loop(0, chunks, own_chunk)

    def carry_on(d, src, ck):
        @pl.when(ck == 0)
        def _():
            pltpu.make_async_copy(meta.at[src], meta.at[src], meta_r.at[src]).wait()

        @pl.when(at_end(d))
        def _():
            landed(pk, (src, slice(None), slice(None), cols(ck)), zr.at[src, ck])
            spread(src, ck)

        @pl.when(jnp.logical_not(at_end(d)))
        def _():
            @pl.when(ck == 0)
            def _():
                build(src, z, src)

                @pl.when(next_end(d))
                def _():
                    build(src, end_of(d), Z + src)

            landed(raw, (src, slice(None), cols(ck)), zr.at[src, ck])

            @pl.when(jnp.logical_not(next_end(d)))
            def _():
                raw_on(d, src, ck).start()

            @pl.when(next_end(d))
            def _():
                epk[src, :, :, cols(ck)] = pack(Z + src, raw[src, :, cols(ck)])
                packed_on(d, src, src, ck).start()

            pk[src, :, :, cols(ck)] = pack(src, raw[src, :, cols(ck)])
            spread(src, ck)

    tile = min(256, hidden)

    def run_expert(src, now):
        def gather(ck):
            landed(xb, (src, slice(None), slice(None), cols(ck)), er.at[src, ck])
            xs[:, cols(ck)] = xb[src, :, :, cols(ck)].reshape(S, part)

        loop(0, chunks, gather)

        def inner(n):
            at = pl.ds(pl.multiple_of(n * tile, tile), tile)
            gated = jnp.minimum(
                jnp.dot(xs[...], gate_w[:, at], preferred_element_type=f32), LIMIT
            )
            linear = jnp.clip(
                jnp.dot(xs[...], up_w[:, at], preferred_element_type=f32), -LIMIT, LIMIT
            )
            act[:, at] = (gated * jax.nn.sigmoid(SLOPE * gated) * (linear + 1.0)).astype(bf16)

        loop(0, hidden // tile, inner)

        def outer(ck):
            result = jnp.dot(act[...], down_w[:, cols(ck)], preferred_element_type=f32)
            xb[src, :, :, cols(ck)] = result.reshape(EP, K, part).astype(bf16)

            if now:
                give_back(src, ck)

        loop(0, chunks, outer)

    def far_slot(d, src):
        return jnp.where(jnp.logical_and(d == 1, z + 1 == src), Z, src)

    def back_packed(d, src, ck):
        return remote(
            rb.at[src, :, :, cols(ck)], fp.at[far_slot(d, src), :, :, cols(ck)],
            fs.at[src, ck], fa.at[far_slot(d, src), ck], side(1 - d),
        )

    def back_raw(d, src, ck):
        return remote(
            raw.at[src, :, cols(ck)], fr.at[far_slot(d, src), :, cols(ck)],
            fs.at[src, ck], fa.at[far_slot(d, src), ck], side(1 - d),
        )

    def add_far(d, slot, ck):
        @pl.when(next_end(d))
        def _():
            landed(fp, (slot, slice(None), slice(None), cols(ck)), fa.at[slot, ck])
            acc[...] += unpack(Z + slot, fp[slot, :, :, cols(ck)])

        @pl.when(jnp.logical_not(next_end(d)))
        def _():
            landed(fr, (slot, slice(None), cols(ck)), fa.at[slot, ck])
            acc[...] += fr[slot, :, cols(ck)].astype(f32)

    def returned(src, ck):
        landed(rb, (src, slice(None), slice(None), cols(ck)), rr.at[src, ck])

    def send_back(d, src, ck):
        returned(src, ck)

        @pl.when(at_end(d))
        def _():
            back_packed(d, src, ck).start()

        @pl.when(jnp.logical_not(at_end(d)))
        def _():
            acc[...] = unpack(src, rb[src, :, :, cols(ck)])
            add_far(d, src, ck)

            @pl.when(jnp.logical_not(next_end(d)))
            def _():
                raw_on(d, src, ck).wait_send()

            raw[src, :, cols(ck)] = acc[...].astype(bf16)
            back_raw(d, src, ck).start()

    def wait_weights():
        for copy in weights:
            copy.wait()

    def backward(k):
        def chunk(ck):
            def one(t):
                d = jnp.where(2 * z >= Z, t, 1 - t)
                src = (Z - 1 - k) * (1 - d) + k * d

                @pl.when((z - src) * toward(d) > 0)
                def _():
                    send_back(d, src, ck)

            loop(0, 2, one)

        loop(0, chunks, chunk)

    def away(s):
        if Z < 3:
            return s
        return jnp.where(jnp.logical_and(is_end, jnp.logical_and(s > 0, s < 3)), 3 - s, s)

    def inward(t):
        return jnp.where(2 * z >= Z, t, 1 - t)

    def within(src):
        return jnp.logical_and(src >= 0, src < Z)

    def stage(s):
        def chunk(ck):
            def one(d):
                src = z - away(s) * toward(d)

                @pl.when(within(src))
                def _():
                    carry_on(d, src, ck)

            loop(0, 2, one)

            @pl.when(jnp.logical_and(s == 1, ck == 0))
            def _():
                wait_weights()

            def expert(far, t, now):
                src = z - far * toward(inward(t))

                @pl.when(within(src))
                def _():
                    run_expert(src, now)

            middle = jnp.logical_and(s > 1, jnp.logical_not(is_end))
            late_end = jnp.logical_and(is_end, s == 3)
            first = jnp.where(is_end, min(1, last), 0)

            @pl.when(jnp.logical_and(jnp.logical_and(s > 1, ck == first), jnp.logical_not(late_end)))
            def _():
                expert(away(s - 1), 0, True)

            @pl.when(jnp.logical_and(middle, ck == min(1, last)))
            def _():
                expert(s - 1, 1, False)

            @pl.when(ck == last)
            def _():
                @pl.when(s == 1)
                def _():
                    loop(0, 2, lambda d: own_packed(d, early, chunks))
                    run_expert(z, False)

                src = z - (s - 1) * toward(inward(1))

                @pl.when(jnp.logical_and(middle, within(src)))
                def _():
                    loop(0, chunks, lambda i: give_back(src, i))

                @pl.when(s == Z)
                def _():
                    if Z > 2:
                        @pl.when(is_end)
                        def _():
                            expert(away(2), 0, True)
                    loop(0, chunks, lambda i: give_back(z, i))

            turn = jnp.where(jnp.logical_and(is_end, s < Z), 0, last)

            @pl.when(jnp.logical_and(s > 2, ck == turn))
            def _():
                backward(s - 1)

        loop(0, chunks, chunk)

    loop(1, Z + 1, stage)
    if Z > 1:
        backward(1)

    def finish(ck):
        returned(z, ck)
        acc[...] = upd_ref[:, cols(ck)].astype(f32) + unpack(z, rb[z, :, :, cols(ck)])

        def beyond(d):
            @pl.when(exists(d))
            def _():
                add_far(d, own_slot(d), ck)

        loop(0, 2, beyond)
        out_ref[:, cols(ck)] = acc[...].astype(bf16)

    loop(0, chunks, finish)

    for j in range(1, Z):
        meta_copy(j).wait_send()

    def sent_all(ck):
        def own_sent(d):
            @pl.when(jnp.logical_and(exists(d), jnp.logical_not(next_end(d))))
            def _():
                own_raw(d, ck).wait_send()

            @pl.when(jnp.logical_and(exists(d), next_end(d)))
            def _():
                packed_on(d, z, own_slot(d), ck).wait_send()

        loop(0, 2, own_sent)

        def per_source(src):
            some = pl.ds(0, EP - 1)
            landed(pk, (src, some, slice(None), cols(ck)), es.at[src, ck])
            landed(xb, (src, some, slice(None), cols(ck)), rs.at[src, ck])
            d = jnp.where(src < z, 0, 1)

            @pl.when(src != z)
            def _():
                @pl.when(at_end(d))
                def _():
                    back_packed(d, src, ck).wait_send()

                @pl.when(jnp.logical_not(at_end(d)))
                def _():
                    back_raw(d, src, ck).wait_send()

                    @pl.when(next_end(d))
                    def _():
                        packed_on(d, src, src, ck).wait_send()

        loop(0, Z, per_source)

    loop(0, chunks, sent_all)


def experts(route_ids, route_weight, normed, updated, gate_matrix, up_matrix, down_matrix):
    sp_count, dp_count = lax.axis_size("sp"), lax.axis_size("dp")
    planes = 4 if sp_count % 4 == 0 else 1
    lanes_x = sp_count // planes
    rows, width = normed.shape
    top = route_ids.shape[1]
    capacity = max(2, 3 * rows * top // (2 * sp_count * dp_count))
    slots = -(-capacity // 8) * 8
    group = lanes_x * dp_count
    padded = -(-group * slots // 128) * 128
    hidden = gate_matrix.shape[1]
    chunks = CHUNKS if width % (128 * CHUNKS) == 0 else 1
    meta = jnp.concatenate([route_ids.astype(jnp.float32), route_weight], axis=1).T
    dma = pltpu.SemaphoreType.DMA
    vmem = pl.BlockSpec(memory_space=pltpu.VMEM)
    hbm = pl.BlockSpec(memory_space=pl.ANY)
    bf16, f32 = jnp.bfloat16, jnp.float32
    return pl.pallas_call(
        functools.partial(experts_kernel, planes, lanes_x, slots),
        name="routed_experts",
        out_shape=jax.ShapeDtypeStruct((rows, width), bf16),
        in_specs=[vmem] * 3 + [hbm] * 3,
        out_specs=vmem,
        scratch_shapes=[
            pltpu.VMEM((planes, 2 * top, rows), f32),
            pltpu.VMEM((planes, rows, width), bf16),
            pltpu.VMEM((planes, group, slots, width), bf16),
            pltpu.VMEM((planes + 1, group, slots, width), bf16),
            pltpu.VMEM((planes, group, slots, width), bf16),
            pltpu.VMEM((planes, group, slots, width), bf16),
            pltpu.VMEM((planes + 1, rows, width), bf16),
            pltpu.VMEM((planes + 1, group, slots, width), bf16),
            pltpu.VMEM((2 * planes + 1, group * slots, rows), bf16),
            pltpu.VMEM((2 * planes + 1, rows, padded), bf16),
            pltpu.VMEM((2 * planes + 1, rows, padded), bf16),
            pltpu.VMEM((rows, rows), bf16),
            pltpu.VMEM((group * slots, width), bf16),
            pltpu.VMEM((group * slots, hidden), bf16),
            pltpu.VMEM((rows, width // chunks), f32),
            pltpu.VMEM(gate_matrix.shape, bf16),
            pltpu.VMEM(up_matrix.shape, bf16),
            pltpu.VMEM(down_matrix.shape, bf16),
            dma((planes,)), dma((planes,)),
            dma((planes + 1, chunks)), dma((planes, chunks)),
            dma((planes, chunks)), dma((planes, chunks)),
            dma((planes, chunks)), dma((planes, chunks)),
            dma((planes, chunks)), dma((planes + 1, chunks)),
            dma((3,)),
        ],
        compiler_params=pltpu.CompilerParams(
            collective_id=1, has_side_effects=True, vmem_limit_bytes=VMEM_BYTES
        ),
    )(meta, normed, updated, gate_matrix, up_matrix, down_matrix)


def per_device(
    resid,
    query,
    keys,
    values,
    q_gain,
    k_gain,
    out_weight,
    norm_gain,
    route_ids,
    route_weight,
    expert_gate,
    expert_up,
    expert_down,
):
    tok_rows = resid.shape[1]
    head_dim = q_gain.shape[0]
    places = lax.axis_index("sp") * tok_rows + jnp.arange(tok_rows, dtype=jnp.int32)
    cosine, sine = turn_tables(places, head_dim)
    updated, normed = attention(
        query[0], keys[0], values[0], q_gain, k_gain, cosine, sine, resid[0], norm_gain, out_weight
    )
    return experts(
        route_ids[0], route_weight[0], normed, updated,
        expert_gate[0], expert_up[0], expert_down[0],
    )[None]


def solution(mesh):
    placed = (
        P("dp", "sp", None),
        P("dp", "sp", None),
        P("dp", "sp", None),
        P("dp", "sp", None),
        P(),
        P(),
        P("dp", None),
        P(),
        P("dp", "sp", None),
        P("dp", "sp", None),
        P(("sp", "dp"), None, None),
        P(("sp", "dp"), None, None),
        P(("sp", "dp"), None, None),
    )
    return jax.shard_map(
        per_device, mesh=mesh, in_specs=placed, out_specs=P("dp", "sp", None), check_vma=False
    )
```

```python
import functools

import jax
import jax.numpy as jnp
from jax import lax
from jax.experimental import pallas as pl
from jax.experimental.pallas import tpu as pltpu
from jax.sharding import PartitionSpec as P

GRID_W = 64
EPSILON = 1e-06
THETA = 10000.0
LIMIT = 7.0
SLOPE = 1.702
LOG2E = 1.4426950408889634
MESH = pl.DeviceIdType.MESH
VMEM_BYTES = 64000000
CHUNKS = 4


def split_of(count, inner):
    return (count // inner, inner) if count % inner == 0 else (count, 1)


def turn_tables(places, head_dim):
    quarter = head_dim // 4
    inverse = THETA ** (-jnp.arange(quarter, dtype=jnp.float32) / quarter)
    row = (places // GRID_W).astype(jnp.float32)[:, None] * inverse[None, :]
    col = (places % GRID_W).astype(jnp.float32)[:, None] * inverse[None, :]
    cosine = jnp.concatenate([jnp.cos(row)] * 2 + [jnp.cos(col)] * 2, axis=-1)
    sine = jnp.concatenate(
        [-jnp.sin(row), jnp.sin(row), -jnp.sin(col), jnp.sin(col)], axis=-1
    )
    return cosine, sine


def attention_kernel(
    planes, lanes_x, outer_dp, inner_dp,
    q_ref, k_ref, v_ref, qg_ref, kg_ref, cos_ref, sin_ref, resid_ref, ng_ref, w_ref,
    upd_ref, normed_ref,
    kall, vall, wall, qt, acc, mx, ls, head_out,
    kx_s, kx_r, kz_s, kz_r, hz_s, hz_r, hx_s, hx_r, vz_s, vz_r, vx_s, vx_r,
    wy_s, wy_r, wc_s, wc_r, loc,
):
    Z, X, Y, C = planes, lanes_x, outer_dp, inner_dp
    rows, head_dim = cos_ref.shape
    q_heads = q_ref.shape[1] // head_dim
    kv_heads = k_ref.shape[1] // head_dim
    group = q_heads // kv_heads
    w_rows = w_ref.shape[0]
    sp, dp = lax.axis_index("sp"), lax.axis_index("dp")
    z, x = sp // X, sp % X
    y, c = dp // C, dp % C
    up_ok, down_ok = z + 1 < Z, z > 0

    barrier = pltpu.get_barrier_semaphore()

    def greet(device):
        pl.semaphore_signal(barrier, inc=1, device_id=device, device_id_type=MESH)

    for j in range(1, X):
        greet((z * X + (x + j) % X, dp))

    @pl.when(up_ok)
    def _():
        greet((sp + X, dp))

    @pl.when(down_ok)
    def _():
        greet((sp - X, dp))

    for j in range(1, Y):
        greet((sp, ((y + j) % Y) * C + c))
    for j in range(1, C):
        greet((sp, y * C + (c + j) % C))

    def krows(block):
        return pl.ds(pl.multiple_of(block * rows, rows), rows)

    def wrows(block):
        return pl.ds(pl.multiple_of(block * w_rows, w_rows), w_rows)

    v_own = pltpu.make_async_copy(v_ref, vall.at[krows(sp)], loc.at[0])
    v_own.start()
    w_own = pltpu.make_async_copy(w_ref, wall.at[wrows(dp)], loc.at[1])
    w_own.start()

    lane = lax.broadcasted_iota(jnp.int32, (rows, head_dim), 1)
    first = lane % (head_dim // 2) < head_dim // 4

    def turned(value, gain):
        value = value.astype(jnp.float32)
        value = value * lax.rsqrt(jnp.mean(value * value, axis=-1, keepdims=True) + EPSILON) * gain
        swapped = jnp.where(
            first,
            pltpu.roll(value, head_dim - head_dim // 4, 1),
            pltpu.roll(value, head_dim // 4, 1),
        )
        return (value * cos_ref[...] + swapped * sin_ref[...]).astype(jnp.bfloat16)

    for g in range(kv_heads):
        span = slice(g * head_dim, (g + 1) * head_dim)
        kall[krows(sp), span] = turned(k_ref[:, span], kg_ref[...])

    count = (X - 1) + (Y - 1) + (C - 1) + up_ok.astype(jnp.int32) + down_ok.astype(jnp.int32)
    v_own.wait()
    w_own.wait()
    pl.semaphore_wait(barrier, count)

    def remote(buf, sl, ssem, rsem, device):
        return pltpu.make_async_remote_copy(
            src_ref=buf.at[sl], dst_ref=buf.at[sl], send_sem=ssem, recv_sem=rsem,
            device_id=device, device_id_type=MESH,
        )

    split = kv_heads // 2 * head_dim
    low, high = slice(0, split), slice(split, kv_heads * head_dim)

    def toward(d):
        return 1 - 2 * d

    def across(j):
        return (z * X + (x + j) % X, dp)

    def onward(d):
        return (sp + X * toward(d), dp)

    def source(d, s):
        return z - s * toward(d)

    def hop(d, s):
        return d * (Z - 1) + s

    def loop(first_index, last_index, body):
        def step(i, carry):
            body(i)
            return carry
        lax.fori_loop(first_index, last_index, step, 0)

    def kx(j):
        return remote(kall, (krows(sp), low), kx_s.at[j], kx_r.at[j], across(j))

    def kz(d, s, j):
        at = hop(d, s) * X + j
        block = source(d, s) * X + (x + X - j) % X
        return remote(kall, (krows(block), low), kz_s.at[at], kz_r.at[at], onward(d))

    def hz(d, s):
        at = hop(d, s)
        return remote(
            kall, (krows(source(d, s) * X + x), high), hz_s.at[at], hz_r.at[at], onward(d)
        )

    def vz(d, s):
        at = hop(d, s)
        return remote(vall, (krows(source(d, s) * X + x),), vz_s.at[at], vz_r.at[at], onward(d))

    def hx(slot, plane, j):
        at = slot * X + j
        return remote(
            kall, (krows(plane * X + x), high), hx_s.at[at], hx_r.at[at], across(j)
        )

    def vx(slot, plane, j):
        at = slot * X + j
        return remote(vall, (krows(plane * X + x),), vx_s.at[at], vx_r.at[at], across(j))

    def valid(plane):
        return jnp.logical_and(plane >= 0, plane < Z)

    def sends(d, s):
        return jnp.logical_and(valid(z + toward(d)), valid(source(d, s)))

    def gets(d, s):
        return valid(source(d, s + 1))

    pieces = wy_s.shape[0] // Y
    w_part = w_rows // pieces

    def wpart(block, h):
        return pl.ds(pl.multiple_of(block * w_rows + h * w_part, w_part), w_part)

    def wy(j, h):
        at = j * pieces + h
        return remote(
            wall, (wpart(dp, h),), wy_s.at[at], wy_r.at[at], (sp, ((y + j) % Y) * C + c)
        )

    def wc(j, i, h):
        at = (j * C + i) * pieces + h
        return remote(
            wall, (wpart(((y + Y - j) % Y) * C + c, h),), wc_s.at[at], wc_r.at[at],
            (sp, y * C + (c + i) % C),
        )

    for j in range(1, X):
        kx(j).start()
    for d in range(2):
        @pl.when(sends(d, 0))
        def _(d=d):
            vz(d, 0).start()
            hz(d, 0).start()
            kz(d, 0, 0).start()
    for j in range(1, X):
        hx(0, z, j).start()
        vx(0, z, j).start()
    for h in range(pieces):
        for j in range(1, Y):
            wy(j, h).start()
        for i in range(1, C):
            wc(0, i, h).start()

    def prepare_queries(h, carry):
        at = pl.ds(pl.multiple_of(h * head_dim, head_dim), head_dim)
        qt[h] = turned(q_ref[:, at], qg_ref[...])
        return carry

    lax.fori_loop(0, q_heads // 4, prepare_queries, 0)
    for j in range(1, X):
        kx(j).wait_recv()
    for d in range(2):
        @pl.when(sends(d, 0))
        def _(d=d):
            for j in range(1, X):
                kz(d, 0, j).start()
    lax.fori_loop(q_heads // 4, q_heads, prepare_queries, 0)

    factor = head_dim ** (-0.5) * LOG2E
    keys_in = X * rows

    def attend(plane, fresh):
        at_rows = pl.ds(pl.multiple_of(plane * keys_in, keys_in), keys_in)

        def one_group(i, carry):
            span = pl.ds(pl.multiple_of(i * head_dim, head_dim), head_dim)
            for u in range(group):
                h = i * group + u
                scores = lax.dot_general(
                    qt[h], kall[at_rows, span], (((1,), (1,)), ((), ())),
                    preferred_element_type=jnp.float32,
                )
                top = jnp.max(scores, axis=-1, keepdims=True)
                if not fresh:
                    before = mx[h]
                    top = jnp.maximum(before[:, :1], top)
                lifted = jnp.exp2((scores - top) * factor)
                total = jnp.sum(lifted, axis=-1, keepdims=True)
                part = jnp.dot(
                    lifted.astype(jnp.bfloat16), vall[at_rows, span],
                    preferred_element_type=jnp.float32,
                )
                wide = jnp.broadcast_to(top, (rows, head_dim))
                wide_total = jnp.broadcast_to(total, (rows, head_dim))
                if fresh:
                    acc[h], ls[h] = part, wide_total
                else:
                    fade = jnp.exp2((before - wide) * factor)
                    acc[h] = acc[h] * fade + part
                    ls[h] = ls[h] * fade + wide_total
                mx[h] = wide
            return carry

        lax.fori_loop(0, kv_heads, one_group, 0)

    def wait_across(slot, plane):
        for j in range(1, X):
            hx(slot, plane, j).wait_recv()
            vx(slot, plane, j).wait_recv()

    def inward(t):
        return jnp.where(2 * z >= Z, t, 1 - t)

    def open_step(s):
        def one(t):
            d = inward(t)

            @pl.when(gets(d, s))
            def _():
                plane, slot = source(d, s + 1), 1 + hop(d, s)
                more = jnp.logical_and(s + 1 < Z - 1, sends(d, s + 1))
                vz(d, s).wait_recv()
                for j in range(1, X):
                    vx(slot, plane, j).start()

                @pl.when(more)
                def _():
                    vz(d, s + 1).start()

                hz(d, s).wait_recv()
                for j in range(1, X):
                    hx(slot, plane, j).start()

                @pl.when(more)
                def _():
                    hz(d, s + 1).start()

        loop(0, 2, one)

    def close_step(s):
        def one(t):
            d = inward(t)

            @pl.when(gets(d, s))
            def _():
                more = jnp.logical_and(s + 1 < Z - 1, sends(d, s + 1))
                for j in range(X):
                    kz(d, s, j).wait_recv()

                    @pl.when(more)
                    def _(j=j):
                        kz(d, s + 1, j).start()

        loop(0, 2, one)

    def pass_weights():
        for h in range(pieces):
            for j in range(1, Y):
                wy(j, h).wait_recv()
                for i in range(1, C):
                    wc(j, i, h).start()

    def walk(s):
        close_step(s)

        @pl.when(s == Z - 2)
        def _():
            pass_weights()

        is_end = jnp.logical_or(z == 0, z == Z - 1)
        turn = jnp.where(is_end, 0, 1)

        def one(t):
            @pl.when(jnp.logical_and(t == turn, s + 1 < Z - 1))
            def _():
                open_step(s + 1)

            d = inward(t)

            @pl.when(gets(d, s))
            def _():
                plane = source(d, s + 1)
                wait_across(1 + hop(d, s), plane)
                attend(plane, False)

        loop(0, 2, one)

    if Z > 1:
        open_step(0)
    wait_across(0, z)
    attend(z, True)
    if Z > 1:
        loop(0, Z - 1, walk)
    else:
        pass_weights()

    for h in range(q_heads):
        head_out[:, h * head_dim:(h + 1) * head_dim] = (acc[h] / ls[h]).astype(jnp.bfloat16)

    for h in range(pieces):
        for j in range(Y):
            for i in range(1, C):
                wc(j, i, h).wait_recv()

    width = wall.shape[1]
    tile = min(256, width)

    def project(n, total):
        at = pl.ds(pl.multiple_of(n * tile, tile), tile)
        projected = jnp.dot(head_out[...], wall[:, at], preferred_element_type=jnp.float32)
        updated = (resid_ref[:, at].astype(jnp.float32) + projected).astype(jnp.bfloat16)
        upd_ref[:, at] = updated
        wide = updated.astype(jnp.float32)
        return total + jnp.sum(wide * wide, axis=-1, keepdims=True)

    square = lax.fori_loop(0, width // tile, project, jnp.zeros((rows, 1), jnp.float32))
    scale = lax.rsqrt(square / width + EPSILON)

    def normalize(n, carry):
        at = pl.ds(pl.multiple_of(n * tile, tile), tile)
        normed_ref[:, at] = (
            upd_ref[:, at].astype(jnp.float32) * scale * ng_ref[:, at]
        ).astype(jnp.bfloat16)
        return carry

    lax.fori_loop(0, width // tile, normalize, 0)

    for j in range(1, X):
        kx(j).wait_send()
        hx(0, z, j).wait_send()
        vx(0, z, j).wait_send()

    def drain(s):
        def one(d):
            @pl.when(sends(d, s))
            def _():
                vz(d, s).wait_send()
                hz(d, s).wait_send()
                for j in range(X):
                    kz(d, s, j).wait_send()

            @pl.when(gets(d, s))
            def _():
                for j in range(1, X):
                    hx(1 + hop(d, s), source(d, s + 1), j).wait_send()
                    vx(1 + hop(d, s), source(d, s + 1), j).wait_send()

        loop(0, 2, one)

    loop(0, Z - 1, drain)
    for h in range(pieces):
        for j in range(1, Y):
            wy(j, h).wait_send()
        for j in range(Y):
            for i in range(1, C):
                wc(j, i, h).wait_send()


def attention(query, keys, values, q_gain, k_gain, cosine, sine, resid, norm_gain, out_weight):
    sp_count, dp_count = lax.axis_size("sp"), lax.axis_size("dp")
    planes = 4 if sp_count % 4 == 0 else 1
    lanes_x = sp_count // planes
    outer_dp, inner_dp = split_of(dp_count, 2)
    rows, head_dim = cosine.shape
    q_heads = query.shape[1] // head_dim
    width = resid.shape[1]
    dma = pltpu.SemaphoreType.DMA
    vmem = pl.BlockSpec(memory_space=pltpu.VMEM)
    hops = 2 * max(planes - 1, 1)
    pieces = 4 if out_weight.shape[0] % 64 == 0 else 1
    full_kv = (sp_count * rows, keys.shape[1])
    return pl.pallas_call(
        functools.partial(attention_kernel, planes, lanes_x, outer_dp, inner_dp),
        name="gathered_attention",
        out_shape=(
            jax.ShapeDtypeStruct((rows, width), jnp.bfloat16),
            jax.ShapeDtypeStruct((rows, width), jnp.bfloat16),
        ),
        in_specs=[vmem, vmem, pl.BlockSpec(memory_space=pl.ANY)]
        + [vmem] * 6
        + [pl.BlockSpec(memory_space=pl.ANY)],
        out_specs=(vmem, vmem),
        scratch_shapes=[
            pltpu.VMEM(full_kv, jnp.bfloat16),
            pltpu.VMEM(full_kv, jnp.bfloat16),
            pltpu.VMEM((dp_count * out_weight.shape[0], width), jnp.bfloat16),
            pltpu.VMEM((q_heads, rows, head_dim), jnp.bfloat16),
            pltpu.VMEM((q_heads, rows, head_dim), jnp.float32),
            pltpu.VMEM((q_heads, rows, head_dim), jnp.float32),
            pltpu.VMEM((q_heads, rows, head_dim), jnp.float32),
            pltpu.VMEM((rows, q_heads * head_dim), jnp.bfloat16),
            dma((lanes_x,)), dma((lanes_x,)),
            dma((hops * lanes_x,)), dma((hops * lanes_x,)),
            dma((hops,)), dma((hops,)),
            dma(((hops + 1) * lanes_x,)), dma(((hops + 1) * lanes_x,)),
            dma((hops,)), dma((hops,)),
            dma(((hops + 1) * lanes_x,)), dma(((hops + 1) * lanes_x,)),
            dma((outer_dp * pieces,)), dma((outer_dp * pieces,)),
            dma((outer_dp * inner_dp * pieces,)), dma((outer_dp * inner_dp * pieces,)),
            dma((2,)),
        ],
        compiler_params=pltpu.CompilerParams(
            collective_id=0, has_side_effects=True, vmem_limit_bytes=VMEM_BYTES
        ),
    )(
        query, keys, values, q_gain[None], k_gain[None], cosine, sine, resid,
        norm_gain[None], out_weight,
    )


def experts_kernel(
    planes, lanes_x, slots,
    meta_ref, normed_ref, upd_ref, gate_hbm, up_hbm, down_hbm,
    out_ref,
    meta, raw, pk, epk, xb, rb, fr, fp, ptab, whi, wlo, tri, xs, act, acc, gate_w, up_w, down_w,
    meta_s, meta_r, zs, zr, es, er, rs, rr, fs, fa, loc,
):
    Z, X, K = planes, lanes_x, slots
    rows, width = normed_ref.shape
    DP = lax.axis_size("dp")
    EP = X * DP
    S = EP * K
    top = meta_ref.shape[0] // 2
    chunks = zr.shape[1]
    part = width // chunks
    hidden = gate_w.shape[1]
    sp, dp = lax.axis_index("sp"), lax.axis_index("dp")
    z, x = sp // X, sp % X
    p = x * DP + dp
    f32, bf16 = jnp.float32, jnp.bfloat16

    def cols(ck):
        return pl.ds(pl.multiple_of(ck * part, part), part)

    def peer(q):
        return (z * X + q // DP, q % DP)

    def loop(low, high, body):
        def step(i, carry):
            body(i)
            return carry
        lax.fori_loop(low, high, step, 0)

    def remote(src, dst, ssem, rsem, device):
        return pltpu.make_async_remote_copy(
            src_ref=src, dst_ref=dst, send_sem=ssem, recv_sem=rsem,
            device_id=device, device_id_type=MESH,
        )

    weights = [
        pltpu.make_async_copy(gate_hbm, gate_w, loc.at[0]),
        pltpu.make_async_copy(up_hbm, up_w, loc.at[1]),
        pltpu.make_async_copy(down_hbm, down_w, loc.at[2]),
    ]

    barrier = pltpu.get_barrier_semaphore()

    def greet(device):
        pl.semaphore_signal(barrier, inc=1, device_id=device, device_id_type=MESH)

    loop(1, EP, lambda j: greet(peer((p + j) % EP)))
    for j in range(1, Z):
        greet((((z + j) % Z) * X + x, dp))
    for copy in weights:
        copy.start()
    tri[...] = (
        lax.broadcasted_iota(jnp.int32, (rows, rows), 0)
        < lax.broadcasted_iota(jnp.int32, (rows, rows), 1)
    ).astype(f32).astype(bf16)
    pl.semaphore_wait(barrier, EP - 1 + Z - 1)

    def toward(d):
        return 1 - 2 * d

    def side(d):
        return (sp + X * toward(d), dp)

    def end_of(d):
        return (Z - 1) * (1 - d)

    def exists(d):
        return jnp.logical_and(z + toward(d) >= 0, z + toward(d) < Z)

    def at_end(d):
        return z == end_of(d)

    def next_end(d):
        return z + toward(d) == end_of(d)

    def own_slot(d):
        return z + d * (Z - z)

    def meta_copy(j):
        return remote(
            meta_ref, meta.at[z], meta_s.at[j], meta_r.at[z], (((z + j) % Z) * X + x, dp)
        )

    def own_raw(d, ck):
        return remote(
            normed_ref.at[:, cols(ck)], raw.at[z, :, cols(ck)],
            zs.at[own_slot(d), ck], zr.at[z, ck], side(d),
        )

    def raw_on(d, src, ck):
        return remote(
            raw.at[src, :, cols(ck)], raw.at[src, :, cols(ck)],
            zs.at[src, ck], zr.at[src, ck], side(d),
        )

    def packed_on(d, src, slot, ck):
        return remote(
            epk.at[slot, :, :, cols(ck)], pk.at[src, :, :, cols(ck)],
            zs.at[slot, ck], zr.at[src, ck], side(d),
        )

    def landed(buf, index, sem):
        view = buf.at[index]
        pltpu.make_async_copy(view, view, sem).wait()

    def spread(src, ck):
        pltpu.make_async_copy(
            pk.at[src, p, :, cols(ck)], xb.at[src, p, :, cols(ck)], er.at[src, ck]
        ).start()

        def one(j):
            q = (p + j) % EP
            remote(
                pk.at[src, q, :, cols(ck)], xb.at[src, p, :, cols(ck)],
                es.at[src, ck], er.at[src, ck], peer(q),
            ).start()

        loop(1, EP, one)

    def give_back(src, ck):
        pltpu.make_async_copy(
            xb.at[src, p, :, cols(ck)], rb.at[src, p, :, cols(ck)], rr.at[src, ck]
        ).start()

        def one(j):
            q = (p + j) % EP
            remote(
                xb.at[src, q, :, cols(ck)], rb.at[src, p, :, cols(ck)],
                rs.at[src, ck], rr.at[src, ck], peer(q),
            ).start()

        loop(1, EP, one)

    def build(src, plane, index):
        info = meta[src]
        lane_expert = (
            lax.broadcasted_iota(jnp.int32, (EP, rows), 0) + plane * EP
        ).astype(f32)
        named = jnp.zeros((EP, rows), f32)
        scale = jnp.zeros((EP, rows), f32)
        for i in range(top):
            hit = info[i:i + 1] == lane_expert
            named = jnp.where(hit, 1.0, named)
            scale = jnp.where(hit, info[top + i:top + i + 1], scale)
        rank = jnp.dot(named.astype(bf16), tri[...], preferred_element_type=f32)
        rank = jnp.where(named > 0.0, rank, -1.0)
        place = lax.broadcasted_iota(jnp.int32, (K, rows), 0).astype(f32)
        ones, scaled = [], []
        for e in range(EP):
            one = jnp.where(rank[e:e + 1] == place, 1.0, 0.0)
            ones.append(one)
            scaled.append(one * scale[e:e + 1])
        ptab[index] = jnp.concatenate(ones, axis=0).astype(bf16)
        spare = whi.shape[2] - S
        if spare:
            scaled.append(jnp.zeros((spare, rows), f32))
        turned = jnp.concatenate(scaled, axis=0).T
        high = turned.astype(bf16)
        whi[index] = high
        wlo[index] = (turned - high.astype(f32)).astype(bf16)

    def pack(index, value):
        got = jnp.dot(ptab[index], value, preferred_element_type=f32)
        return got.reshape(EP, K, part).astype(bf16)

    def unpack(index, value):
        flat = value.reshape(S, part)
        return jnp.dot(whi[index, :, :S], flat, preferred_element_type=f32) + jnp.dot(
            wlo[index, :, :S], flat, preferred_element_type=f32
        )

    for j in range(1, Z):
        meta_copy(j).start()

    def own_raw_start(d):
        @pl.when(jnp.logical_and(exists(d), jnp.logical_not(next_end(d))))
        def _():
            loop(0, chunks, lambda ck: own_raw(d, ck).start())

    loop(0, 2, own_raw_start)
    meta[z] = meta_ref[...]

    def own_packed(d, low, high):
        @pl.when(jnp.logical_and(exists(d), next_end(d)))
        def _():
            slot = own_slot(d)

            def chunk(ck):
                epk[slot, :, :, cols(ck)] = pack(Z + slot, normed_ref[:, cols(ck)])
                packed_on(d, z, slot, ck).start()

            loop(low, high, chunk)

    def own_packed_start(d):
        @pl.when(jnp.logical_and(exists(d), next_end(d)))
        def _():
            build(z, end_of(d), Z + own_slot(d))

        own_packed(d, 0, early)

    early = -(-chunks // 2)
    last = chunks - 1
    is_end = jnp.logical_or(z == 0, z == Z - 1)
    loop(0, 2, own_packed_start)
    build(z, z, z)

    def own_chunk(ck):
        pk[z, :, :, cols(ck)] = pack(z, normed_ref[:, cols(ck)])
        spread(z, ck)

    loop(0, chunks, own_chunk)

    def carry_on(d, src, ck):
        @pl.when(ck == 0)
        def _():
            pltpu.make_async_copy(meta.at[src], meta.at[src], meta_r.at[src]).wait()

        @pl.when(at_end(d))
        def _():
            landed(pk, (src, slice(None), slice(None), cols(ck)), zr.at[src, ck])
            spread(src, ck)

        @pl.when(jnp.logical_not(at_end(d)))
        def _():
            @pl.when(ck == 0)
            def _():
                build(src, z, src)

                @pl.when(next_end(d))
                def _():
                    build(src, end_of(d), Z + src)

            landed(raw, (src, slice(None), cols(ck)), zr.at[src, ck])

            @pl.when(jnp.logical_not(next_end(d)))
            def _():
                raw_on(d, src, ck).start()

            @pl.when(next_end(d))
            def _():
                epk[src, :, :, cols(ck)] = pack(Z + src, raw[src, :, cols(ck)])
                packed_on(d, src, src, ck).start()

            pk[src, :, :, cols(ck)] = pack(src, raw[src, :, cols(ck)])
            spread(src, ck)

    tile = min(256, hidden)

    def run_expert(src, now):
        def gather(ck):
            landed(xb, (src, slice(None), slice(None), cols(ck)), er.at[src, ck])
            xs[:, cols(ck)] = xb[src, :, :, cols(ck)].reshape(S, part)

        loop(0, chunks, gather)

        def inner(n):
            at = pl.ds(pl.multiple_of(n * tile, tile), tile)
            gated = jnp.minimum(
                jnp.dot(xs[...], gate_w[:, at], preferred_element_type=f32), LIMIT
            )
            linear = jnp.clip(
                jnp.dot(xs[...], up_w[:, at], preferred_element_type=f32), -LIMIT, LIMIT
            )
            act[:, at] = (gated * jax.nn.sigmoid(SLOPE * gated) * (linear + 1.0)).astype(bf16)

        loop(0, hidden // tile, inner)

        def outer(ck):
            result = jnp.dot(act[...], down_w[:, cols(ck)], preferred_element_type=f32)
            xb[src, :, :, cols(ck)] = result.reshape(EP, K, part).astype(bf16)

            if now:
                give_back(src, ck)

        loop(0, chunks, outer)

    def far_slot(d, src):
        return jnp.where(jnp.logical_and(d == 1, z + 1 == src), Z, src)

    def back_packed(d, src, ck):
        return remote(
            rb.at[src, :, :, cols(ck)], fp.at[far_slot(d, src), :, :, cols(ck)],
            fs.at[src, ck], fa.at[far_slot(d, src), ck], side(1 - d),
        )

    def back_raw(d, src, ck):
        return remote(
            raw.at[src, :, cols(ck)], fr.at[far_slot(d, src), :, cols(ck)],
            fs.at[src, ck], fa.at[far_slot(d, src), ck], side(1 - d),
        )

    def add_far(d, slot, ck):
        @pl.when(next_end(d))
        def _():
            landed(fp, (slot, slice(None), slice(None), cols(ck)), fa.at[slot, ck])
            acc[...] += unpack(Z + slot, fp[slot, :, :, cols(ck)])

        @pl.when(jnp.logical_not(next_end(d)))
        def _():
            landed(fr, (slot, slice(None), cols(ck)), fa.at[slot, ck])
            acc[...] += fr[slot, :, cols(ck)].astype(f32)

    def returned(src, ck):
        landed(rb, (src, slice(None), slice(None), cols(ck)), rr.at[src, ck])

    def send_back(d, src, ck):
        returned(src, ck)

        @pl.when(at_end(d))
        def _():
            back_packed(d, src, ck).start()

        @pl.when(jnp.logical_not(at_end(d)))
        def _():
            acc[...] = unpack(src, rb[src, :, :, cols(ck)])
            add_far(d, src, ck)

            @pl.when(jnp.logical_not(next_end(d)))
            def _():
                raw_on(d, src, ck).wait_send()

            raw[src, :, cols(ck)] = acc[...].astype(bf16)
            back_raw(d, src, ck).start()

    def wait_weights():
        for copy in weights:
            copy.wait()

    def backward(k):
        def chunk(ck):
            def one(t):
                d = jnp.where(2 * z >= Z, t, 1 - t)
                src = (Z - 1 - k) * (1 - d) + k * d

                @pl.when((z - src) * toward(d) > 0)
                def _():
                    send_back(d, src, ck)

            loop(0, 2, one)

        loop(0, chunks, chunk)

    def away(s):
        if Z < 3:
            return s
        return jnp.where(jnp.logical_and(is_end, jnp.logical_and(s > 0, s < 3)), 3 - s, s)

    def inward(t):
        return jnp.where(2 * z >= Z, t, 1 - t)

    def within(src):
        return jnp.logical_and(src >= 0, src < Z)

    def stage(s):
        def chunk(ck):
            def one(d):
                src = z - away(s) * toward(d)

                @pl.when(within(src))
                def _():
                    carry_on(d, src, ck)

            loop(0, 2, one)

            @pl.when(jnp.logical_and(s == 1, ck == 0))
            def _():
                wait_weights()

            def expert(far, t, now):
                src = z - far * toward(inward(t))

                @pl.when(within(src))
                def _():
                    run_expert(src, now)

            middle = jnp.logical_and(s > 1, jnp.logical_not(is_end))
            late_end = jnp.logical_and(is_end, s == 3)
            first = jnp.where(is_end, min(1, last), 0)

            @pl.when(jnp.logical_and(jnp.logical_and(s > 1, ck == first), jnp.logical_not(late_end)))
            def _():
                expert(away(s - 1), 0, True)

            @pl.when(jnp.logical_and(middle, ck == min(1, last)))
            def _():
                expert(s - 1, 1, False)

            @pl.when(ck == last)
            def _():
                @pl.when(s == 1)
                def _():
                    loop(0, 2, lambda d: own_packed(d, early, chunks))
                    run_expert(z, False)

                src = z - (s - 1) * toward(inward(1))

                @pl.when(jnp.logical_and(middle, within(src)))
                def _():
                    loop(0, chunks, lambda i: give_back(src, i))

                @pl.when(s == Z)
                def _():
                    if Z > 2:
                        @pl.when(is_end)
                        def _():
                            expert(away(2), 0, True)
                    loop(0, chunks, lambda i: give_back(z, i))

            turn = jnp.where(jnp.logical_and(is_end, s < Z), 0, last)

            @pl.when(jnp.logical_and(s > 2, ck == turn))
            def _():
                backward(s - 1)

        loop(0, chunks, chunk)

    loop(1, Z + 1, stage)
    if Z > 1:
        backward(1)

    def finish(ck):
        returned(z, ck)
        acc[...] = upd_ref[:, cols(ck)].astype(f32) + unpack(z, rb[z, :, :, cols(ck)])

        def beyond(d):
            @pl.when(exists(d))
            def _():
                add_far(d, own_slot(d), ck)

        loop(0, 2, beyond)
        out_ref[:, cols(ck)] = acc[...].astype(bf16)

    loop(0, chunks, finish)

    for j in range(1, Z):
        meta_copy(j).wait_send()

    def sent_all(ck):
        def own_sent(d):
            @pl.when(jnp.logical_and(exists(d), jnp.logical_not(next_end(d))))
            def _():
                own_raw(d, ck).wait_send()

            @pl.when(jnp.logical_and(exists(d), next_end(d)))
            def _():
                packed_on(d, z, own_slot(d), ck).wait_send()

        loop(0, 2, own_sent)

        def per_source(src):
            some = pl.ds(0, EP - 1)
            landed(pk, (src, some, slice(None), cols(ck)), es.at[src, ck])
            landed(xb, (src, some, slice(None), cols(ck)), rs.at[src, ck])
            d = jnp.where(src < z, 0, 1)

            @pl.when(src != z)
            def _():
                @pl.when(at_end(d))
                def _():
                    back_packed(d, src, ck).wait_send()

                @pl.when(jnp.logical_not(at_end(d)))
                def _():
                    back_raw(d, src, ck).wait_send()

                    @pl.when(next_end(d))
                    def _():
                        packed_on(d, src, src, ck).wait_send()

        loop(0, Z, per_source)

    loop(0, chunks, sent_all)


def experts(route_ids, route_weight, normed, updated, gate_matrix, up_matrix, down_matrix):
    sp_count, dp_count = lax.axis_size("sp"), lax.axis_size("dp")
    planes = 4 if sp_count % 4 == 0 else 1
    lanes_x = sp_count // planes
    rows, width = normed.shape
    top = route_ids.shape[1]
    capacity = max(2, 3 * rows * top // (2 * sp_count * dp_count))
    slots = -(-capacity // 8) * 8
    group = lanes_x * dp_count
    padded = -(-group * slots // 128) * 128
    hidden = gate_matrix.shape[1]
    chunks = CHUNKS if width % (128 * CHUNKS) == 0 else 1
    meta = jnp.concatenate([route_ids.astype(jnp.float32), route_weight], axis=1).T
    dma = pltpu.SemaphoreType.DMA
    vmem = pl.BlockSpec(memory_space=pltpu.VMEM)
    hbm = pl.BlockSpec(memory_space=pl.ANY)
    bf16, f32 = jnp.bfloat16, jnp.float32
    return pl.pallas_call(
        functools.partial(experts_kernel, planes, lanes_x, slots),
        name="routed_experts",
        out_shape=jax.ShapeDtypeStruct((rows, width), bf16),
        in_specs=[vmem] * 3 + [hbm] * 3,
        out_specs=vmem,
        scratch_shapes=[
            pltpu.VMEM((planes, 2 * top, rows), f32),
            pltpu.VMEM((planes, rows, width), bf16),
            pltpu.VMEM((planes, group, slots, width), bf16),
            pltpu.VMEM((planes + 1, group, slots, width), bf16),
            pltpu.VMEM((planes, group, slots, width), bf16),
            pltpu.VMEM((planes, group, slots, width), bf16),
            pltpu.VMEM((planes + 1, rows, width), bf16),
            pltpu.VMEM((planes + 1, group, slots, width), bf16),
            pltpu.VMEM((2 * planes + 1, group * slots, rows), bf16),
            pltpu.VMEM((2 * planes + 1, rows, padded), bf16),
            pltpu.VMEM((2 * planes + 1, rows, padded), bf16),
            pltpu.VMEM((rows, rows), bf16),
            pltpu.VMEM((group * slots, width), bf16),
            pltpu.VMEM((group * slots, hidden), bf16),
            pltpu.VMEM((rows, width // chunks), f32),
            pltpu.VMEM(gate_matrix.shape, bf16),
            pltpu.VMEM(up_matrix.shape, bf16),
            pltpu.VMEM(down_matrix.shape, bf16),
            dma((planes,)), dma((planes,)),
            dma((planes + 1, chunks)), dma((planes, chunks)),
            dma((planes, chunks)), dma((planes, chunks)),
            dma((planes, chunks)), dma((planes, chunks)),
            dma((planes, chunks)), dma((planes + 1, chunks)),
            dma((3,)),
        ],
        compiler_params=pltpu.CompilerParams(
            collective_id=1, has_side_effects=True, vmem_limit_bytes=VMEM_BYTES
        ),
    )(meta, normed, updated, gate_matrix, up_matrix, down_matrix)


def per_device(
    resid,
    query,
    keys,
    values,
    q_gain,
    k_gain,
    out_weight,
    norm_gain,
    route_ids,
    route_weight,
    expert_gate,
    expert_up,
    expert_down,
):
    tok_rows = resid.shape[1]
    head_dim = q_gain.shape[0]
    places = lax.axis_index("sp") * tok_rows + jnp.arange(tok_rows, dtype=jnp.int32)
    cosine, sine = turn_tables(places, head_dim)
    updated, normed = attention(
        query[0], keys[0], values[0], q_gain, k_gain, cosine, sine, resid[0], norm_gain, out_weight
    )
    return experts(
        route_ids[0], route_weight[0], normed, updated,
        expert_gate[0], expert_up[0], expert_down[0],
    )[None]


def solution(mesh):
    placed = (
        P("dp", "sp", None),
        P("dp", "sp", None),
        P("dp", "sp", None),
        P("dp", "sp", None),
        P(),
        P(),
        P("dp", None),
        P(),
        P("dp", "sp", None),
        P("dp", "sp", None),
        P(("sp", "dp"), None, None),
        P(("sp", "dp"), None, None),
        P(("sp", "dp"), None, None),
    )
    return jax.shard_map(
        per_device, mesh=mesh, in_specs=placed, out_specs=P("dp", "sp", None), check_vma=False
    )
```

```python
import functools

import jax
import jax.numpy as jnp
from jax import lax
from jax.experimental import pallas as pl
from jax.experimental.pallas import tpu as pltpu
from jax.sharding import PartitionSpec as P

GRID_W = 64
EPSILON = 1e-06
THETA = 10000.0
LIMIT = 7.0
SLOPE = 1.702
LOG2E = 1.4426950408889634
MESH = pl.DeviceIdType.MESH
VMEM_BYTES = 64000000
CHUNKS = 4


def split_of(count, inner):
    return (count // inner, inner) if count % inner == 0 else (count, 1)


def turn_tables(places, head_dim):
    quarter = head_dim // 4
    lane = jnp.arange(head_dim, dtype=jnp.int32)[None, :]
    inverse = THETA ** (-(lane % quarter).astype(jnp.float32) / quarter)
    row, col = places[:, None] // GRID_W, places[:, None] % GRID_W
    angle = jnp.where(lane < 2 * quarter, row, col).astype(jnp.float32) * inverse
    sign = jnp.where(lane % (2 * quarter) < quarter, -1.0, 1.0)
    return jnp.cos(angle), jnp.sin(angle) * sign


def attention_kernel(
    planes, lanes_x, outer_dp, inner_dp,
    q_hbm, k_ref, v_ref, qg_ref, kg_ref, cos_ref, sin_ref, resid_hbm, ng_ref, w_ref,
    upd_ref, normed_ref,
    q_ref, resid_ref, kall, vall, wall, qt, acc, mx, ls, head_out,
    kx_s, kx_r, kz_s, kz_r, hz_s, hz_r, hx_s, hx_r, vz_s, vz_r, vx_s, vx_r,
    wy_s, wy_r, wc_s, wc_r, loc,
):
    Z, X, Y, C = planes, lanes_x, outer_dp, inner_dp
    rows, head_dim = cos_ref.shape
    q_heads = q_ref.shape[1] // head_dim
    kv_heads = k_ref.shape[1] // head_dim
    group = q_heads // kv_heads
    w_rows = w_ref.shape[0]
    sp, dp = lax.axis_index("sp"), lax.axis_index("dp")
    z, x = sp // X, sp % X
    y, c = dp // C, dp % C
    up_ok, down_ok = z + 1 < Z, z > 0

    barrier = pltpu.get_barrier_semaphore()

    def greet(device):
        pl.semaphore_signal(barrier, inc=1, device_id=device, device_id_type=MESH)

    for j in range(1, X):
        greet((z * X + (x + j) % X, dp))

    @pl.when(up_ok)
    def _():
        greet((sp + X, dp))

    @pl.when(down_ok)
    def _():
        greet((sp - X, dp))

    for j in range(1, Y):
        greet((sp, ((y + j) % Y) * C + c))
    for j in range(1, C):
        greet((sp, y * C + (c + j) % C))

    def krows(block):
        return pl.ds(pl.multiple_of(block * rows, rows), rows)

    def wrows(block):
        return pl.ds(pl.multiple_of(block * w_rows, w_rows), w_rows)

    v_own = pltpu.make_async_copy(v_ref, vall.at[krows(sp)], loc.at[0])
    v_own.start()
    w_own = pltpu.make_async_copy(w_ref, wall.at[wrows(dp)], loc.at[1])
    w_own.start()
    q_own = pltpu.make_async_copy(q_hbm, q_ref, loc.at[2])
    q_own.start()
    resid_own = pltpu.make_async_copy(resid_hbm, resid_ref, loc.at[3])
    resid_own.start()

    lane = lax.broadcasted_iota(jnp.int32, (rows, head_dim), 1)
    first = lane % (head_dim // 2) < head_dim // 4

    def turned(value, gain):
        value = value.astype(jnp.float32)
        value = value * lax.rsqrt(jnp.mean(value * value, axis=-1, keepdims=True) + EPSILON) * gain
        swapped = jnp.where(
            first,
            pltpu.roll(value, head_dim - head_dim // 4, 1),
            pltpu.roll(value, head_dim // 4, 1),
        )
        return (value * cos_ref[...] + swapped * sin_ref[...]).astype(jnp.bfloat16)

    for g in range(kv_heads):
        span = slice(g * head_dim, (g + 1) * head_dim)
        kall[krows(sp), span] = turned(k_ref[:, span], kg_ref[...])

    count = (X - 1) + (Y - 1) + (C - 1) + up_ok.astype(jnp.int32) + down_ok.astype(jnp.int32)
    v_own.wait()
    w_own.wait()
    pl.semaphore_wait(barrier, count)

    def remote(buf, sl, ssem, rsem, device):
        return pltpu.make_async_remote_copy(
            src_ref=buf.at[sl], dst_ref=buf.at[sl], send_sem=ssem, recv_sem=rsem,
            device_id=device, device_id_type=MESH,
        )

    split = kv_heads // 2 * head_dim
    low, high = slice(0, split), slice(split, kv_heads * head_dim)

    def toward(d):
        return 1 - 2 * d

    def across(j):
        return (z * X + (x + j) % X, dp)

    def onward(d):
        return (sp + X * toward(d), dp)

    def source(d, s):
        return z - s * toward(d)

    def hop(d, s):
        return d * (Z - 1) + s

    def loop(first_index, last_index, body):
        def step(i, carry):
            body(i)
            return carry
        lax.fori_loop(first_index, last_index, step, 0)

    def kx(j):
        return remote(kall, (krows(sp), low), kx_s.at[j], kx_r.at[j], across(j))

    def kz(d, s, j):
        at = hop(d, s) * X + j
        block = source(d, s) * X + (x + X - j) % X
        return remote(kall, (krows(block), low), kz_s.at[at], kz_r.at[at], onward(d))

    def hz(d, s):
        at = hop(d, s)
        return remote(
            kall, (krows(source(d, s) * X + x), high), hz_s.at[at], hz_r.at[at], onward(d)
        )

    def vz(d, s):
        at = hop(d, s)
        return remote(vall, (krows(source(d, s) * X + x),), vz_s.at[at], vz_r.at[at], onward(d))

    def hx(slot, plane, j):
        at = slot * X + j
        return remote(
            kall, (krows(plane * X + x), high), hx_s.at[at], hx_r.at[at], across(j)
        )

    def vx(slot, plane, j):
        at = slot * X + j
        return remote(vall, (krows(plane * X + x),), vx_s.at[at], vx_r.at[at], across(j))

    def valid(plane):
        return jnp.logical_and(plane >= 0, plane < Z)

    def sends(d, s):
        return jnp.logical_and(valid(z + toward(d)), valid(source(d, s)))

    def gets(d, s):
        return valid(source(d, s + 1))

    pieces = wy_s.shape[0] // Y
    w_part = w_rows // pieces

    def wpart(block, h):
        return pl.ds(pl.multiple_of(block * w_rows + h * w_part, w_part), w_part)

    def wy(j, h):
        at = j * pieces + h
        return remote(
            wall, (wpart(dp, h),), wy_s.at[at], wy_r.at[at], (sp, ((y + j) % Y) * C + c)
        )

    def wc(j, i, h):
        at = (j * C + i) * pieces + h
        return remote(
            wall, (wpart(((y + Y - j) % Y) * C + c, h),), wc_s.at[at], wc_r.at[at],
            (sp, y * C + (c + i) % C),
        )

    for j in range(1, X):
        kx(j).start()
    for d in range(2):
        @pl.when(sends(d, 0))
        def _(d=d):
            vz(d, 0).start()
            hz(d, 0).start()
            kz(d, 0, 0).start()
    for j in range(1, X):
        hx(0, z, j).start()
        vx(0, z, j).start()
    for h in range(pieces):
        for j in range(1, Y):
            wy(j, h).start()
        for i in range(1, C):
            wc(0, i, h).start()

    def prepare_queries(h, carry):
        at = pl.ds(pl.multiple_of(h * head_dim, head_dim), head_dim)
        qt[h] = turned(q_ref[:, at], qg_ref[...])
        return carry

    q_own.wait()
    lax.fori_loop(0, q_heads // 4, prepare_queries, 0)
    for j in range(1, X):
        kx(j).wait_recv()
    for d in range(2):
        @pl.when(sends(d, 0))
        def _(d=d):
            for j in range(1, X):
                kz(d, 0, j).start()
    lax.fori_loop(q_heads // 4, q_heads, prepare_queries, 0)

    factor = head_dim ** (-0.5) * LOG2E
    keys_in = X * rows

    def attend(plane, fresh):
        at_rows = pl.ds(pl.multiple_of(plane * keys_in, keys_in), keys_in)

        def one_group(i, carry):
            span = pl.ds(pl.multiple_of(i * head_dim, head_dim), head_dim)
            for u in range(group):
                h = i * group + u
                scores = lax.dot_general(
                    qt[h], kall[at_rows, span], (((1,), (1,)), ((), ())),
                    preferred_element_type=jnp.float32,
                )
                top = jnp.max(scores, axis=-1, keepdims=True)
                if not fresh:
                    before = mx[h]
                    top = jnp.maximum(before[:, :1], top)
                lifted = jnp.exp2((scores - top) * factor)
                total = jnp.sum(lifted, axis=-1, keepdims=True)
                part = jnp.dot(
                    lifted.astype(jnp.bfloat16), vall[at_rows, span],
                    preferred_element_type=jnp.float32,
                )
                wide = jnp.broadcast_to(top, (rows, head_dim))
                wide_total = jnp.broadcast_to(total, (rows, head_dim))
                if fresh:
                    acc[h], ls[h] = part, wide_total
                else:
                    fade = jnp.exp2((before - wide) * factor)
                    acc[h] = acc[h] * fade + part
                    ls[h] = ls[h] * fade + wide_total
                mx[h] = wide
            return carry

        lax.fori_loop(0, kv_heads, one_group, 0)

    def wait_across(slot, plane):
        for j in range(1, X):
            hx(slot, plane, j).wait_recv()
            vx(slot, plane, j).wait_recv()

    def inward(t):
        return jnp.where(2 * z >= Z, t, 1 - t)

    def open_step(s):
        def one(t):
            d = inward(t)

            @pl.when(gets(d, s))
            def _():
                plane, slot = source(d, s + 1), 1 + hop(d, s)
                more = jnp.logical_and(s + 1 < Z - 1, sends(d, s + 1))
                vz(d, s).wait_recv()
                for j in range(1, X):
                    vx(slot, plane, j).start()

                @pl.when(more)
                def _():
                    vz(d, s + 1).start()

                hz(d, s).wait_recv()
                for j in range(1, X):
                    hx(slot, plane, j).start()

                @pl.when(more)
                def _():
                    hz(d, s + 1).start()

        loop(0, 2, one)

    def close_step(s):
        def one(t):
            d = inward(t)

            @pl.when(gets(d, s))
            def _():
                more = jnp.logical_and(s + 1 < Z - 1, sends(d, s + 1))
                for j in range(X):
                    kz(d, s, j).wait_recv()

                    @pl.when(more)
                    def _(j=j):
                        kz(d, s + 1, j).start()

        loop(0, 2, one)

    def pass_weights():
        for h in range(pieces):
            for j in range(1, Y):
                wy(j, h).wait_recv()
                for i in range(1, C):
                    wc(j, i, h).start()

    def walk(s):
        close_step(s)

        @pl.when(s == Z - 2)
        def _():
            pass_weights()

        is_end = jnp.logical_or(z == 0, z == Z - 1)
        turn = jnp.where(is_end, 0, 1)

        def one(t):
            @pl.when(jnp.logical_and(t == turn, s + 1 < Z - 1))
            def _():
                open_step(s + 1)

            d = inward(t)

            @pl.when(gets(d, s))
            def _():
                plane = source(d, s + 1)
                wait_across(1 + hop(d, s), plane)
                attend(plane, False)

        loop(0, 2, one)

    if Z > 1:
        open_step(0)
    wait_across(0, z)
    attend(z, True)
    if Z > 1:
        loop(0, Z - 1, walk)
    else:
        pass_weights()

    for h in range(q_heads):
        head_out[:, h * head_dim:(h + 1) * head_dim] = (acc[h] / ls[h]).astype(jnp.bfloat16)

    for h in range(pieces):
        for j in range(Y):
            for i in range(1, C):
                wc(j, i, h).wait_recv()

    resid_own.wait()
    width = wall.shape[1]
    tile = min(256, width)

    def project(n, total):
        at = pl.ds(pl.multiple_of(n * tile, tile), tile)
        projected = jnp.dot(head_out[...], wall[:, at], preferred_element_type=jnp.float32)
        updated = (resid_ref[:, at].astype(jnp.float32) + projected).astype(jnp.bfloat16)
        upd_ref[:, at] = updated
        wide = updated.astype(jnp.float32)
        return total + jnp.sum(wide * wide, axis=-1, keepdims=True)

    square = lax.fori_loop(0, width // tile, project, jnp.zeros((rows, 1), jnp.float32))
    scale = lax.rsqrt(square / width + EPSILON)

    def normalize(n, carry):
        at = pl.ds(pl.multiple_of(n * tile, tile), tile)
        normed_ref[:, at] = (
            upd_ref[:, at].astype(jnp.float32) * scale * ng_ref[:, at]
        ).astype(jnp.bfloat16)
        return carry

    lax.fori_loop(0, width // tile, normalize, 0)

    for j in range(1, X):
        kx(j).wait_send()
        hx(0, z, j).wait_send()
        vx(0, z, j).wait_send()

    def drain(s):
        def one(d):
            @pl.when(sends(d, s))
            def _():
                vz(d, s).wait_send()
                hz(d, s).wait_send()
                for j in range(X):
                    kz(d, s, j).wait_send()

            @pl.when(gets(d, s))
            def _():
                for j in range(1, X):
                    hx(1 + hop(d, s), source(d, s + 1), j).wait_send()
                    vx(1 + hop(d, s), source(d, s + 1), j).wait_send()

        loop(0, 2, one)

    loop(0, Z - 1, drain)
    for h in range(pieces):
        for j in range(1, Y):
            wy(j, h).wait_send()
        for j in range(Y):
            for i in range(1, C):
                wc(j, i, h).wait_send()


def attention(query, keys, values, q_gain, k_gain, cosine, sine, resid, norm_gain, out_weight):
    sp_count, dp_count = lax.axis_size("sp"), lax.axis_size("dp")
    planes = 4 if sp_count % 4 == 0 else 1
    lanes_x = sp_count // planes
    outer_dp, inner_dp = split_of(dp_count, 2)
    rows, head_dim = cosine.shape
    q_heads = query.shape[1] // head_dim
    width = resid.shape[1]
    dma = pltpu.SemaphoreType.DMA
    vmem = pl.BlockSpec(memory_space=pltpu.VMEM)
    hops = 2 * max(planes - 1, 1)
    pieces = 4 if out_weight.shape[0] % 64 == 0 else 1
    full_kv = (sp_count * rows, keys.shape[1])
    hbm = pl.BlockSpec(memory_space=pl.ANY)
    return pl.pallas_call(
        functools.partial(attention_kernel, planes, lanes_x, outer_dp, inner_dp),
        name="gathered_attention",
        out_shape=(
            jax.ShapeDtypeStruct((rows, width), jnp.bfloat16),
            jax.ShapeDtypeStruct((rows, width), jnp.bfloat16),
        ),
        in_specs=[hbm, vmem, hbm] + [vmem] * 4 + [hbm, vmem, hbm],
        out_specs=(vmem, vmem),
        scratch_shapes=[
            pltpu.VMEM(query.shape, jnp.bfloat16),
            pltpu.VMEM(resid.shape, jnp.bfloat16),
            pltpu.VMEM(full_kv, jnp.bfloat16),
            pltpu.VMEM(full_kv, jnp.bfloat16),
            pltpu.VMEM((dp_count * out_weight.shape[0], width), jnp.bfloat16),
            pltpu.VMEM((q_heads, rows, head_dim), jnp.bfloat16),
            pltpu.VMEM((q_heads, rows, head_dim), jnp.float32),
            pltpu.VMEM((q_heads, rows, head_dim), jnp.float32),
            pltpu.VMEM((q_heads, rows, head_dim), jnp.float32),
            pltpu.VMEM((rows, q_heads * head_dim), jnp.bfloat16),
            dma((lanes_x,)), dma((lanes_x,)),
            dma((hops * lanes_x,)), dma((hops * lanes_x,)),
            dma((hops,)), dma((hops,)),
            dma(((hops + 1) * lanes_x,)), dma(((hops + 1) * lanes_x,)),
            dma((hops,)), dma((hops,)),
            dma(((hops + 1) * lanes_x,)), dma(((hops + 1) * lanes_x,)),
            dma((outer_dp * pieces,)), dma((outer_dp * pieces,)),
            dma((outer_dp * inner_dp * pieces,)), dma((outer_dp * inner_dp * pieces,)),
            dma((4,)),
        ],
        compiler_params=pltpu.CompilerParams(
            collective_id=0, has_side_effects=True, vmem_limit_bytes=VMEM_BYTES
        ),
    )(
        query, keys, values, q_gain[None], k_gain[None], cosine, sine, resid,
        norm_gain[None], out_weight,
    )


def experts_kernel(
    planes, lanes_x, slots,
    ids_ref, scale_ref, normed_ref, upd_hbm, gate_hbm, up_hbm, down_hbm,
    out_ref,
    meta, upd_ref, raw, pk, epk, xb, rb, fr, fp, ptab, whi, wlo, tri, xs, sums, act, acc, gate_w, up_w, down_w,
    meta_s, meta_r, zs, zr, es, er, rs, rr, fs, fa, loc,
):
    Z, X, K = planes, lanes_x, slots
    rows, width = normed_ref.shape
    DP = lax.axis_size("dp")
    EP = X * DP
    S = EP * K
    top = ids_ref.shape[0]
    chunks = zr.shape[1]
    part = width // chunks
    hidden = gate_w.shape[1]
    sp, dp = lax.axis_index("sp"), lax.axis_index("dp")
    z, x = sp // X, sp % X
    p = x * DP + dp
    f32, bf16 = jnp.float32, jnp.bfloat16

    def cols(ck):
        return pl.ds(pl.multiple_of(ck * part, part), part)

    def peer(q):
        return (z * X + q // DP, q % DP)

    def loop(low, high, body):
        def step(i, carry):
            body(i)
            return carry
        lax.fori_loop(low, high, step, 0)

    def remote(src, dst, ssem, rsem, device):
        return pltpu.make_async_remote_copy(
            src_ref=src, dst_ref=dst, send_sem=ssem, recv_sem=rsem,
            device_id=device, device_id_type=MESH,
        )

    weights = [
        pltpu.make_async_copy(gate_hbm, gate_w, loc.at[0]),
        pltpu.make_async_copy(up_hbm, up_w, loc.at[1]),
        pltpu.make_async_copy(down_hbm, down_w, loc.at[2]),
    ]

    barrier = pltpu.get_barrier_semaphore()

    def greet(device):
        pl.semaphore_signal(barrier, inc=1, device_id=device, device_id_type=MESH)

    loop(1, EP, lambda j: greet(peer((p + j) % EP)))
    for j in range(1, Z):
        greet((((z + j) % Z) * X + x, dp))
    for copy in weights:
        copy.start()
    upd_copy = pltpu.make_async_copy(upd_hbm, upd_ref, loc.at[3])
    upd_copy.start()
    meta[z, :top] = ids_ref[...].astype(f32)
    meta[z, top:] = scale_ref[...]
    tri[...] = (
        lax.broadcasted_iota(jnp.int32, (rows, rows), 0)
        < lax.broadcasted_iota(jnp.int32, (rows, rows), 1)
    ).astype(f32).astype(bf16)
    pl.semaphore_wait(barrier, EP - 1 + Z - 1)

    def toward(d):
        return 1 - 2 * d

    def side(d):
        return (sp + X * toward(d), dp)

    def end_of(d):
        return (Z - 1) * (1 - d)

    def exists(d):
        return jnp.logical_and(z + toward(d) >= 0, z + toward(d) < Z)

    def at_end(d):
        return z == end_of(d)

    def next_end(d):
        return z + toward(d) == end_of(d)

    def own_slot(d):
        return z + d * (Z - z)

    def meta_copy(j):
        return remote(
            meta.at[z], meta.at[z], meta_s.at[j], meta_r.at[z], (((z + j) % Z) * X + x, dp)
        )

    def own_raw(d, ck):
        return remote(
            normed_ref.at[:, cols(ck)], raw.at[z, :, cols(ck)],
            zs.at[own_slot(d), ck], zr.at[z, ck], side(d),
        )

    def raw_on(d, src, ck):
        return remote(
            raw.at[src, :, cols(ck)], raw.at[src, :, cols(ck)],
            zs.at[src, ck], zr.at[src, ck], side(d),
        )

    def packed_on(d, src, slot, ck):
        return remote(
            epk.at[slot, :, :, cols(ck)], pk.at[src, :, :, cols(ck)],
            zs.at[slot, ck], zr.at[src, ck], side(d),
        )

    def landed(buf, index, sem):
        view = buf.at[index]
        pltpu.make_async_copy(view, view, sem).wait()

    def spread(src, ck):
        pltpu.make_async_copy(
            pk.at[src, p, :, cols(ck)], xb.at[src, p, :, cols(ck)], er.at[src, ck]
        ).start()

        def one(j):
            q = (p + j) % EP
            remote(
                pk.at[src, q, :, cols(ck)], xb.at[src, p, :, cols(ck)],
                es.at[src, ck], er.at[src, ck], peer(q),
            ).start()

        loop(1, EP, one)

    def give_back(src, ck):
        pltpu.make_async_copy(
            xb.at[src, p, :, cols(ck)], rb.at[src, p, :, cols(ck)], rr.at[src, ck]
        ).start()

        def one(j):
            q = (p + j) % EP
            remote(
                xb.at[src, q, :, cols(ck)], rb.at[src, p, :, cols(ck)],
                rs.at[src, ck], rr.at[src, ck], peer(q),
            ).start()

        loop(1, EP, one)

    def build(src, plane, index):
        info = meta[src]
        lane_expert = (
            lax.broadcasted_iota(jnp.int32, (EP, rows), 0) + plane * EP
        ).astype(f32)
        named = jnp.zeros((EP, rows), f32)
        scale = jnp.zeros((EP, rows), f32)
        for i in range(top):
            hit = info[i:i + 1] == lane_expert
            named = jnp.where(hit, 1.0, named)
            scale = jnp.where(hit, info[top + i:top + i + 1], scale)
        rank = jnp.dot(named.astype(bf16), tri[...], preferred_element_type=f32)
        rank = jnp.where(named > 0.0, rank, -1.0)
        place = lax.broadcasted_iota(jnp.int32, (K, rows), 0).astype(f32)
        ones, scaled = [], []
        for e in range(EP):
            one = jnp.where(rank[e:e + 1] == place, 1.0, 0.0)
            ones.append(one)
            scaled.append(one * scale[e:e + 1])
        ptab[index] = jnp.concatenate(ones, axis=0).astype(bf16)
        spare = whi.shape[2] - S
        if spare:
            scaled.append(jnp.zeros((spare, rows), f32))
        turned = jnp.concatenate(scaled, axis=0).T
        high = turned.astype(bf16)
        whi[index] = high
        wlo[index] = (turned - high.astype(f32)).astype(bf16)

    def pack(index, value):
        got = jnp.dot(ptab[index], value, preferred_element_type=f32)
        return got.reshape(EP, K, part).astype(bf16)

    def unpack(index, value):
        flat = value.reshape(S, part)
        return jnp.dot(whi[index, :, :S], flat, preferred_element_type=f32) + jnp.dot(
            wlo[index, :, :S], flat, preferred_element_type=f32
        )

    for j in range(1, Z):
        meta_copy(j).start()

    def own_raw_start(d):
        @pl.when(jnp.logical_and(exists(d), jnp.logical_not(next_end(d))))
        def _():
            loop(0, chunks, lambda ck: own_raw(d, ck).start())

    loop(0, 2, own_raw_start)

    def own_packed(d, low, high):
        @pl.when(jnp.logical_and(exists(d), next_end(d)))
        def _():
            slot = own_slot(d)

            def chunk(ck):
                epk[slot, :, :, cols(ck)] = pack(Z + slot, normed_ref[:, cols(ck)])
                packed_on(d, z, slot, ck).start()

            loop(low, high, chunk)

    def own_packed_start(d):
        @pl.when(jnp.logical_and(exists(d), next_end(d)))
        def _():
            build(z, end_of(d), Z + own_slot(d))

        own_packed(d, 0, early)

    early = -(-chunks // 2)
    last = chunks - 1
    is_end = jnp.logical_or(z == 0, z == Z - 1)
    loop(0, 2, own_packed_start)
    build(z, z, z)

    def own_chunk(ck):
        pk[z, :, :, cols(ck)] = pack(z, normed_ref[:, cols(ck)])
        spread(z, ck)

    loop(0, chunks, own_chunk)

    def held(src, ck):
        near = jnp.logical_or(src == z + 1, src == z - 1)
        return jnp.logical_and(near, ck >= early) if Z > 2 else False

    def carry_on(d, src, ck):
        @pl.when(ck == 0)
        def _():
            pltpu.make_async_copy(meta.at[src], meta.at[src], meta_r.at[src]).wait()

        @pl.when(at_end(d))
        def _():
            landed(pk, (src, slice(None), slice(None), cols(ck)), zr.at[src, ck])

            @pl.when(jnp.logical_not(held(src, ck)))
            def _():
                spread(src, ck)

        @pl.when(jnp.logical_not(at_end(d)))
        def _():
            @pl.when(ck == 0)
            def _():
                build(src, z, src)

                @pl.when(next_end(d))
                def _():
                    build(src, end_of(d), Z + src)

            landed(raw, (src, slice(None), cols(ck)), zr.at[src, ck])

            @pl.when(jnp.logical_not(next_end(d)))
            def _():
                raw_on(d, src, ck).start()

            @pl.when(next_end(d))
            def _():
                epk[src, :, :, cols(ck)] = pack(Z + src, raw[src, :, cols(ck)])
                packed_on(d, src, src, ck).start()

            pk[src, :, :, cols(ck)] = pack(src, raw[src, :, cols(ck)])
            spread(src, ck)

    tile = min(256, hidden)

    def run_expert(src, now):
        def gather(ck):
            landed(xb, (src, slice(None), slice(None), cols(ck)), er.at[src, ck])
            xs[:, cols(ck)] = xb[src, :, :, cols(ck)].reshape(S, part)

        def products(at, low, high):
            span = slice(low * part, high * part)
            return [
                jnp.dot(xs[:, span], matrix[span, at], preferred_element_type=f32)
                for matrix in (gate_w, up_w)
            ]

        def spot(n):
            return pl.ds(pl.multiple_of(n * tile, tile), tile)

        def begin(n):
            for i, value in enumerate(products(spot(n), 0, chunks - 1)):
                sums[i, :, spot(n)] = value

        def inner(n):
            values = products(spot(n), chunks - 1 if chunks > 1 else 0, chunks)
            if chunks > 1:
                values = [value + sums[i, :, spot(n)] for i, value in enumerate(values)]
            gated = jnp.minimum(values[0], LIMIT)
            linear = jnp.clip(values[1], -LIMIT, LIMIT)
            act[:, spot(n)] = (
                gated * jax.nn.sigmoid(SLOPE * gated) * (linear + 1.0)
            ).astype(bf16)

        if chunks > 1:
            loop(0, chunks - 1, gather)
            loop(0, hidden // tile, begin)
        gather(chunks - 1)
        loop(0, hidden // tile, inner)

        def outer(ck):
            result = jnp.dot(act[...], down_w[:, cols(ck)], preferred_element_type=f32)
            xb[src, :, :, cols(ck)] = result.reshape(EP, K, part).astype(bf16)

            if now:
                give_back(src, ck)

        loop(0, chunks, outer)

    def far_slot(d, src):
        return jnp.where(jnp.logical_and(d == 1, z + 1 == src), Z, src)

    def back_packed(d, src, ck):
        return remote(
            rb.at[src, :, :, cols(ck)], fp.at[far_slot(d, src), :, :, cols(ck)],
            fs.at[src, ck], fa.at[far_slot(d, src), ck], side(1 - d),
        )

    def back_raw(d, src, ck):
        return remote(
            raw.at[src, :, cols(ck)], fr.at[far_slot(d, src), :, cols(ck)],
            fs.at[src, ck], fa.at[far_slot(d, src), ck], side(1 - d),
        )

    def add_far(d, slot, ck):
        @pl.when(next_end(d))
        def _():
            landed(fp, (slot, slice(None), slice(None), cols(ck)), fa.at[slot, ck])
            acc[...] += unpack(Z + slot, fp[slot, :, :, cols(ck)])

        @pl.when(jnp.logical_not(next_end(d)))
        def _():
            landed(fr, (slot, slice(None), cols(ck)), fa.at[slot, ck])
            acc[...] += fr[slot, :, cols(ck)].astype(f32)

    def returned(src, ck):
        landed(rb, (src, slice(None), slice(None), cols(ck)), rr.at[src, ck])

    def send_back(d, src, ck):
        returned(src, ck)

        @pl.when(at_end(d))
        def _():
            back_packed(d, src, ck).start()

        @pl.when(jnp.logical_not(at_end(d)))
        def _():
            acc[...] = unpack(src, rb[src, :, :, cols(ck)])
            add_far(d, src, ck)

            @pl.when(jnp.logical_not(next_end(d)))
            def _():
                raw_on(d, src, ck).wait_send()

            raw[src, :, cols(ck)] = acc[...].astype(bf16)
            back_raw(d, src, ck).start()

    def wait_weights():
        for copy in weights:
            copy.wait()

    def backward(k, low, high):
        def turn(i):
            def one(t):
                d, ck = inward(t), i - t
                src = (Z - 1 - k) * (1 - d) + k * d
                ready = jnp.logical_and(ck >= low, ck < high)

                @pl.when(jnp.logical_and(ready, (z - src) * toward(d) > 0))
                def _():
                    send_back(d, src, ck)

            loop(0, 2, one)

        loop(low, high + 1, turn)

    def away(s):
        if Z < 3:
            return s
        return jnp.where(jnp.logical_and(is_end, jnp.logical_and(s > 0, s < 3)), 3 - s, s)

    def inward(t):
        return jnp.where(2 * z >= Z, t, 1 - t)

    def within(src):
        return jnp.logical_and(src >= 0, src < Z)

    def stage(s):
        def chunk(ck):
            def one(d):
                src = z - away(s) * toward(d)

                @pl.when(within(src))
                def _():
                    carry_on(d, src, ck)

            loop(0, 2, one)

            @pl.when(jnp.logical_and(s == 1, ck == 0))
            def _():
                wait_weights()

            def expert(far, t, now):
                src = z - far * toward(inward(t))

                @pl.when(within(src))
                def _():
                    run_expert(src, now)

            middle = jnp.logical_and(s > 1, jnp.logical_not(is_end))
            late_end = jnp.logical_and(is_end, s == 3)
            first = jnp.where(is_end, min(1, last), 0)

            lead = jnp.logical_and(jnp.logical_and(s > 2, s < Z), ck == 0)

            @pl.when(jnp.logical_and(lead, jnp.logical_not(is_end)))
            def _():
                backward(s - 1, 0, 1)

            @pl.when(jnp.logical_and(jnp.logical_and(s > 1, ck == first), jnp.logical_not(late_end)))
            def _():
                expert(away(s - 1), 0, True)

            @pl.when(jnp.logical_and(middle, ck == min(1, last)))
            def _():
                expert(s - 1, 1, False)

            @pl.when(ck == last)
            def _():
                @pl.when(s == 1)
                def _():
                    loop(0, 2, lambda d: own_packed(d, early, chunks))
                    run_expert(z, False)

                if Z > 2:
                    @pl.when(jnp.logical_and(is_end, s == Z - 1))
                    def _():
                        beside = jnp.where(z == 0, 1, Z - 2)
                        loop(early, chunks, lambda i: spread(beside, i))

                src = z - (s - 1) * toward(inward(1))

                @pl.when(jnp.logical_and(middle, within(src)))
                def _():
                    loop(0, chunks, lambda i: give_back(src, i))

                @pl.when(s == Z)
                def _():
                    loop(0, chunks, lambda i: give_back(z, i))

            ahead = jnp.where(s < Z, 1, 0)
            turn = jnp.where(jnp.logical_and(is_end, s < Z), 0, last)

            @pl.when(jnp.logical_and(s > 2, ck == turn))
            def _():
                backward(s - 1, jnp.where(is_end, 0, ahead), chunks)

            if Z > 2:
                @pl.when(jnp.logical_and(jnp.logical_and(s == Z, ck == last), is_end))
                def _():
                    expert(away(2), 0, True)

        loop(0, chunks, chunk)

    loop(1, Z + 1, stage)
    if Z > 1:
        backward(1, 0, chunks)

    upd_copy.wait()

    def finish(ck):
        returned(z, ck)
        acc[...] = upd_ref[:, cols(ck)].astype(f32) + unpack(z, rb[z, :, :, cols(ck)])

        def beyond(d):
            @pl.when(exists(d))
            def _():
                add_far(d, own_slot(d), ck)

        loop(0, 2, beyond)
        out_ref[:, cols(ck)] = acc[...].astype(bf16)

    loop(0, chunks, finish)

    for j in range(1, Z):
        meta_copy(j).wait_send()

    def sent_all(ck):
        def own_sent(d):
            @pl.when(jnp.logical_and(exists(d), jnp.logical_not(next_end(d))))
            def _():
                own_raw(d, ck).wait_send()

            @pl.when(jnp.logical_and(exists(d), next_end(d)))
            def _():
                packed_on(d, z, own_slot(d), ck).wait_send()

        loop(0, 2, own_sent)

        def per_source(src):
            some = pl.ds(0, EP - 1)
            landed(pk, (src, some, slice(None), cols(ck)), es.at[src, ck])
            landed(xb, (src, some, slice(None), cols(ck)), rs.at[src, ck])
            d = jnp.where(src < z, 0, 1)

            @pl.when(src != z)
            def _():
                @pl.when(at_end(d))
                def _():
                    back_packed(d, src, ck).wait_send()

                @pl.when(jnp.logical_not(at_end(d)))
                def _():
                    back_raw(d, src, ck).wait_send()

                    @pl.when(next_end(d))
                    def _():
                        packed_on(d, src, src, ck).wait_send()

        loop(0, Z, per_source)

    loop(0, chunks, sent_all)


def experts(route_ids, route_weight, normed, updated, gate_matrix, up_matrix, down_matrix):
    sp_count, dp_count = lax.axis_size("sp"), lax.axis_size("dp")
    planes = 4 if sp_count % 4 == 0 else 1
    lanes_x = sp_count // planes
    rows, width = normed.shape
    top = route_ids.shape[1]
    capacity = max(2, 3 * rows * top // (2 * sp_count * dp_count))
    slots = -(-capacity // 8) * 8
    group = lanes_x * dp_count
    padded = -(-group * slots // 128) * 128
    hidden = gate_matrix.shape[1]
    chunks = CHUNKS if width % (128 * CHUNKS) == 0 else 1
    dma = pltpu.SemaphoreType.DMA
    vmem = pl.BlockSpec(memory_space=pltpu.VMEM)
    hbm = pl.BlockSpec(memory_space=pl.ANY)
    bf16, f32 = jnp.bfloat16, jnp.float32
    return pl.pallas_call(
        functools.partial(experts_kernel, planes, lanes_x, slots),
        name="routed_experts",
        out_shape=jax.ShapeDtypeStruct((rows, width), bf16),
        in_specs=[vmem] * 3 + [hbm] * 4,
        out_specs=vmem,
        scratch_shapes=[
            pltpu.VMEM((planes, 2 * top, rows), f32),
            pltpu.VMEM((rows, width), bf16),
            pltpu.VMEM((planes, rows, width), bf16),
            pltpu.VMEM((planes, group, slots, width), bf16),
            pltpu.VMEM((planes + 1, group, slots, width), bf16),
            pltpu.VMEM((planes, group, slots, width), bf16),
            pltpu.VMEM((planes, group, slots, width), bf16),
            pltpu.VMEM((planes + 1, rows, width), bf16),
            pltpu.VMEM((planes + 1, group, slots, width), bf16),
            pltpu.VMEM((2 * planes + 1, group * slots, rows), bf16),
            pltpu.VMEM((2 * planes + 1, rows, padded), bf16),
            pltpu.VMEM((2 * planes + 1, rows, padded), bf16),
            pltpu.VMEM((rows, rows), bf16),
            pltpu.VMEM((group * slots, width), bf16),
            pltpu.VMEM((2, group * slots, hidden), f32),
            pltpu.VMEM((group * slots, hidden), bf16),
            pltpu.VMEM((rows, width // chunks), f32),
            pltpu.VMEM(gate_matrix.shape, bf16),
            pltpu.VMEM(up_matrix.shape, bf16),
            pltpu.VMEM(down_matrix.shape, bf16),
            dma((planes,)), dma((planes,)),
            dma((planes + 1, chunks)), dma((planes, chunks)),
            dma((planes, chunks)), dma((planes, chunks)),
            dma((planes, chunks)), dma((planes, chunks)),
            dma((planes, chunks)), dma((planes + 1, chunks)),
            dma((4,)),
        ],
        compiler_params=pltpu.CompilerParams(
            collective_id=1, has_side_effects=True, vmem_limit_bytes=VMEM_BYTES
        ),
    )(route_ids.T, route_weight.T, normed, updated, gate_matrix, up_matrix, down_matrix)


def per_device(
    resid,
    query,
    keys,
    values,
    q_gain,
    k_gain,
    out_weight,
    norm_gain,
    route_ids,
    route_weight,
    expert_gate,
    expert_up,
    expert_down,
):
    tok_rows = resid.shape[1]
    head_dim = q_gain.shape[0]
    places = lax.axis_index("sp") * tok_rows + jnp.arange(tok_rows, dtype=jnp.int32)
    cosine, sine = turn_tables(places, head_dim)
    updated, normed = attention(
        query[0], keys[0], values[0], q_gain, k_gain, cosine, sine, resid[0], norm_gain, out_weight
    )
    return experts(
        route_ids[0], route_weight[0], normed, updated,
        expert_gate[0], expert_up[0], expert_down[0],
    )[None]


def solution(mesh):
    placed = (
        P("dp", "sp", None),
        P("dp", "sp", None),
        P("dp", "sp", None),
        P("dp", "sp", None),
        P(),
        P(),
        P("dp", None),
        P(),
        P("dp", "sp", None),
        P("dp", "sp", None),
        P(("sp", "dp"), None, None),
        P(("sp", "dp"), None, None),
        P(("sp", "dp"), None, None),
    )
    return jax.shard_map(
        per_device, mesh=mesh, in_specs=placed, out_specs=P("dp", "sp", None), check_vma=False
    )
```

```python
import functools

import jax
import jax.numpy as jnp
from jax import lax
from jax.experimental import pallas as pl
from jax.experimental.pallas import tpu as pltpu
from jax.sharding import PartitionSpec as P

GRID_W = 64
EPSILON = 1e-06
THETA = 10000.0
LIMIT = 7.0
SLOPE = 1.702
LOG2E = 1.4426950408889634
MESH = pl.DeviceIdType.MESH
VMEM_BYTES = 64000000
CHUNKS = 4


def split_of(count, inner):
    return (count // inner, inner) if count % inner == 0 else (count, 1)


def turn_tables(places, head_dim):
    quarter = head_dim // 4
    lane = jnp.arange(head_dim, dtype=jnp.int32)[None, :]
    inverse = THETA ** (-(lane % quarter).astype(jnp.float32) / quarter)
    row, col = places[:, None] // GRID_W, places[:, None] % GRID_W
    angle = jnp.where(lane < 2 * quarter, row, col).astype(jnp.float32) * inverse
    sign = jnp.where(lane % (2 * quarter) < quarter, -1.0, 1.0)
    return jnp.cos(angle), jnp.sin(angle) * sign


def attention_kernel(
    planes, lanes_x, outer_dp, inner_dp,
    q_hbm, k_ref, v_ref, qg_ref, kg_ref, cos_ref, sin_ref, resid_hbm, ng_ref, w_ref,
    upd_ref, normed_ref,
    q_ref, resid_ref, kall, vall, wall, qt, acc, mx, ls, head_out,
    kx_s, kx_r, kz_s, kz_r, hz_s, hz_r, hx_s, hx_r, vz_s, vz_r, vx_s, vx_r,
    wy_s, wy_r, wc_s, wc_r, loc,
):
    Z, X, Y, C = planes, lanes_x, outer_dp, inner_dp
    rows, head_dim = cos_ref.shape
    q_heads = q_ref.shape[1] // head_dim
    kv_heads = k_ref.shape[1] // head_dim
    group = q_heads // kv_heads
    w_rows = w_ref.shape[0]
    sp, dp = lax.axis_index("sp"), lax.axis_index("dp")
    z, x = sp // X, sp % X
    y, c = dp // C, dp % C
    up_ok, down_ok = z + 1 < Z, z > 0

    barrier = pltpu.get_barrier_semaphore()

    def greet(device):
        pl.semaphore_signal(barrier, inc=1, device_id=device, device_id_type=MESH)

    for j in range(1, X):
        greet((z * X + (x + j) % X, dp))

    @pl.when(up_ok)
    def _():
        greet((sp + X, dp))

    @pl.when(down_ok)
    def _():
        greet((sp - X, dp))

    for j in range(1, Y):
        greet((sp, ((y + j) % Y) * C + c))
    for j in range(1, C):
        greet((sp, y * C + (c + j) % C))

    def krows(block):
        return pl.ds(pl.multiple_of(block * rows, rows), rows)

    def wrows(block):
        return pl.ds(pl.multiple_of(block * w_rows, w_rows), w_rows)

    v_own = pltpu.make_async_copy(v_ref, vall.at[krows(sp)], loc.at[0])
    v_own.start()
    w_own = pltpu.make_async_copy(w_ref, wall.at[wrows(dp)], loc.at[1])
    w_own.start()
    q_own = pltpu.make_async_copy(q_hbm, q_ref, loc.at[2])
    q_own.start()
    resid_own = pltpu.make_async_copy(resid_hbm, resid_ref, loc.at[3])
    resid_own.start()

    lane = lax.broadcasted_iota(jnp.int32, (rows, head_dim), 1)
    first = lane % (head_dim // 2) < head_dim // 4

    def turned(value, gain):
        value = value.astype(jnp.float32)
        value = value * lax.rsqrt(jnp.mean(value * value, axis=-1, keepdims=True) + EPSILON) * gain
        swapped = jnp.where(
            first,
            pltpu.roll(value, head_dim - head_dim // 4, 1),
            pltpu.roll(value, head_dim // 4, 1),
        )
        return (value * cos_ref[...] + swapped * sin_ref[...]).astype(jnp.bfloat16)

    for g in range(kv_heads):
        span = slice(g * head_dim, (g + 1) * head_dim)
        kall[krows(sp), span] = turned(k_ref[:, span], kg_ref[...])

    count = (X - 1) + (Y - 1) + (C - 1) + up_ok.astype(jnp.int32) + down_ok.astype(jnp.int32)
    v_own.wait()
    w_own.wait()
    pl.semaphore_wait(barrier, count)

    def remote(buf, sl, ssem, rsem, device):
        return pltpu.make_async_remote_copy(
            src_ref=buf.at[sl], dst_ref=buf.at[sl], send_sem=ssem, recv_sem=rsem,
            device_id=device, device_id_type=MESH,
        )

    split = kv_heads // 2 * head_dim
    low, high = slice(0, split), slice(split, kv_heads * head_dim)

    def toward(d):
        return 1 - 2 * d

    def across(j):
        return (z * X + (x + j) % X, dp)

    def onward(d):
        return (sp + X * toward(d), dp)

    def source(d, s):
        return z - s * toward(d)

    def hop(d, s):
        return d * (Z - 1) + s

    def loop(first_index, last_index, body):
        def step(i, carry):
            body(i)
            return carry
        lax.fori_loop(first_index, last_index, step, 0)

    def kx(j):
        return remote(kall, (krows(sp), low), kx_s.at[j], kx_r.at[j], across(j))

    def kz(d, s, j):
        at = hop(d, s) * X + j
        block = source(d, s) * X + (x + X - j) % X
        return remote(kall, (krows(block), low), kz_s.at[at], kz_r.at[at], onward(d))

    def hz(d, s):
        at = hop(d, s)
        return remote(
            kall, (krows(source(d, s) * X + x), high), hz_s.at[at], hz_r.at[at], onward(d)
        )

    def vz(d, s):
        at = hop(d, s)
        return remote(vall, (krows(source(d, s) * X + x),), vz_s.at[at], vz_r.at[at], onward(d))

    def hx(slot, plane, j):
        at = slot * X + j
        return remote(
            kall, (krows(plane * X + x), high), hx_s.at[at], hx_r.at[at], across(j)
        )

    def vx(slot, plane, j):
        at = slot * X + j
        return remote(vall, (krows(plane * X + x),), vx_s.at[at], vx_r.at[at], across(j))

    def valid(plane):
        return jnp.logical_and(plane >= 0, plane < Z)

    def sends(d, s):
        return jnp.logical_and(valid(z + toward(d)), valid(source(d, s)))

    def gets(d, s):
        return valid(source(d, s + 1))

    pieces = wy_s.shape[0] // Y
    w_part = w_rows // pieces

    def wpart(block, h):
        return pl.ds(pl.multiple_of(block * w_rows + h * w_part, w_part), w_part)

    def wy(j, h):
        at = j * pieces + h
        return remote(
            wall, (wpart(dp, h),), wy_s.at[at], wy_r.at[at], (sp, ((y + j) % Y) * C + c)
        )

    def wc(j, i, h):
        at = (j * C + i) * pieces + h
        return remote(
            wall, (wpart(((y + Y - j) % Y) * C + c, h),), wc_s.at[at], wc_r.at[at],
            (sp, y * C + (c + i) % C),
        )

    for j in range(1, X):
        kx(j).start()
    for d in range(2):
        @pl.when(sends(d, 0))
        def _(d=d):
            vz(d, 0).start()
            hz(d, 0).start()
            kz(d, 0, 0).start()
    for j in range(1, X):
        hx(0, z, j).start()
        vx(0, z, j).start()
    for h in range(pieces):
        for j in range(1, Y):
            wy(j, h).start()
        for i in range(1, C):
            wc(0, i, h).start()

    def prepare_queries(h, carry):
        at = pl.ds(pl.multiple_of(h * head_dim, head_dim), head_dim)
        qt[h] = turned(q_ref[:, at], qg_ref[...])
        return carry

    q_own.wait()
    lax.fori_loop(0, q_heads // 4, prepare_queries, 0)
    for j in range(1, X):
        kx(j).wait_recv()
    for d in range(2):
        @pl.when(sends(d, 0))
        def _(d=d):
            for j in range(1, X):
                kz(d, 0, j).start()
    lax.fori_loop(q_heads // 4, q_heads, prepare_queries, 0)

    factor = head_dim ** (-0.5) * LOG2E
    keys_in = X * rows

    def attend(plane, fresh, begin, end):
        at_rows = pl.ds(pl.multiple_of(plane * keys_in, keys_in), keys_in)

        def one_group(i, carry):
            span = pl.ds(pl.multiple_of(i * head_dim, head_dim), head_dim)
            for u in range(group):
                h = i * group + u
                scores = lax.dot_general(
                    qt[h], kall[at_rows, span], (((1,), (1,)), ((), ())),
                    preferred_element_type=jnp.float32,
                )
                top = jnp.max(scores, axis=-1, keepdims=True)
                if not fresh:
                    before = mx[h]
                    top = jnp.maximum(before[:, :1], top)
                lifted = jnp.exp2((scores - top) * factor)
                total = jnp.sum(lifted, axis=-1, keepdims=True)
                part = jnp.dot(
                    lifted.astype(jnp.bfloat16), vall[at_rows, span],
                    preferred_element_type=jnp.float32,
                )
                wide = jnp.broadcast_to(top, (rows, head_dim))
                wide_total = jnp.broadcast_to(total, (rows, head_dim))
                if fresh:
                    acc[h], ls[h] = part, wide_total
                else:
                    fade = jnp.exp2((before - wide) * factor)
                    acc[h] = acc[h] * fade + part
                    ls[h] = ls[h] * fade + wide_total
                mx[h] = wide
            return carry

        lax.fori_loop(begin, end, one_group, 0)

    def wait_across(slot, plane):
        for j in range(1, X):
            hx(slot, plane, j).wait_recv()
            vx(slot, plane, j).wait_recv()

    def inward(t):
        return jnp.where(2 * z >= Z, t, 1 - t)

    def open_step(s):
        def one(t):
            d = inward(t)

            @pl.when(gets(d, s))
            def _():
                plane, slot = source(d, s + 1), 1 + hop(d, s)
                more = jnp.logical_and(s + 1 < Z - 1, sends(d, s + 1))
                vz(d, s).wait_recv()
                for j in range(1, X):
                    vx(slot, plane, j).start()

                @pl.when(more)
                def _():
                    vz(d, s + 1).start()

                hz(d, s).wait_recv()
                for j in range(1, X):
                    hx(slot, plane, j).start()

                @pl.when(more)
                def _():
                    hz(d, s + 1).start()

        loop(0, 2, one)

    def close_step(s):
        def one(t):
            d = inward(t)

            @pl.when(gets(d, s))
            def _():
                more = jnp.logical_and(s + 1 < Z - 1, sends(d, s + 1))
                for j in range(X):
                    kz(d, s, j).wait_recv()

                    @pl.when(more)
                    def _(j=j):
                        kz(d, s + 1, j).start()

        loop(0, 2, one)

    def pass_weights():
        for h in range(pieces):
            for j in range(1, Y):
                wy(j, h).wait_recv()
                for i in range(1, C):
                    wc(j, i, h).start()

    def walk(s):
        close_step(s)

        is_end = jnp.logical_or(z == 0, z == Z - 1)
        final = s == Z - 2

        @pl.when(jnp.logical_and(final, jnp.logical_not(is_end)))
        def _():
            pass_weights()

        middle = max(kv_heads // 2, 1)
        turn = jnp.where(is_end, 0, 1)

        def one(t):
            @pl.when(jnp.logical_and(t == turn, s + 1 < Z - 1))
            def _():
                open_step(s + 1)

            d = inward(t)

            @pl.when(gets(d, s))
            def _():
                plane = source(d, s + 1)
                wait_across(1 + hop(d, s), plane)

                def part(u):
                    attend(plane, False, u * middle, jnp.where(u == 0, middle, kv_heads))

                    @pl.when(jnp.logical_and(jnp.logical_and(final, is_end), u == 0))
                    def _():
                        pass_weights()

                loop(0, 2, part)

        loop(0, 2, one)

    if Z > 1:
        open_step(0)
    wait_across(0, z)
    attend(z, True, 0, kv_heads)
    if Z > 1:
        loop(0, Z - 1, walk)
    else:
        pass_weights()

    for h in range(q_heads):
        head_out[:, h * head_dim:(h + 1) * head_dim] = (acc[h] / ls[h]).astype(jnp.bfloat16)

    for h in range(pieces):
        for j in range(Y):
            for i in range(1, C):
                wc(j, i, h).wait_recv()

    resid_own.wait()
    width = wall.shape[1]
    tile = min(256, width)

    def project(n, total):
        at = pl.ds(pl.multiple_of(n * tile, tile), tile)
        projected = jnp.dot(head_out[...], wall[:, at], preferred_element_type=jnp.float32)
        updated = (resid_ref[:, at].astype(jnp.float32) + projected).astype(jnp.bfloat16)
        upd_ref[:, at] = updated
        wide = updated.astype(jnp.float32)
        return total + jnp.sum(wide * wide, axis=-1, keepdims=True)

    square = lax.fori_loop(0, width // tile, project, jnp.zeros((rows, 1), jnp.float32))
    scale = lax.rsqrt(square / width + EPSILON)

    def normalize(n, carry):
        at = pl.ds(pl.multiple_of(n * tile, tile), tile)
        normed_ref[:, at] = (
            upd_ref[:, at].astype(jnp.float32) * scale * ng_ref[:, at]
        ).astype(jnp.bfloat16)
        return carry

    lax.fori_loop(0, width // tile, normalize, 0)

    for j in range(1, X):
        kx(j).wait_send()
        hx(0, z, j).wait_send()
        vx(0, z, j).wait_send()

    def drain(s):
        def one(d):
            @pl.when(sends(d, s))
            def _():
                vz(d, s).wait_send()
                hz(d, s).wait_send()
                for j in range(X):
                    kz(d, s, j).wait_send()

            @pl.when(gets(d, s))
            def _():
                for j in range(1, X):
                    hx(1 + hop(d, s), source(d, s + 1), j).wait_send()
                    vx(1 + hop(d, s), source(d, s + 1), j).wait_send()

        loop(0, 2, one)

    loop(0, Z - 1, drain)
    for h in range(pieces):
        for j in range(1, Y):
            wy(j, h).wait_send()
        for j in range(Y):
            for i in range(1, C):
                wc(j, i, h).wait_send()


def attention(query, keys, values, q_gain, k_gain, cosine, sine, resid, norm_gain, out_weight):
    sp_count, dp_count = lax.axis_size("sp"), lax.axis_size("dp")
    planes = 4 if sp_count % 4 == 0 else 1
    lanes_x = sp_count // planes
    outer_dp, inner_dp = split_of(dp_count, 2)
    rows, head_dim = cosine.shape
    q_heads = query.shape[1] // head_dim
    width = resid.shape[1]
    dma = pltpu.SemaphoreType.DMA
    vmem = pl.BlockSpec(memory_space=pltpu.VMEM)
    hops = 2 * max(planes - 1, 1)
    pieces = 4 if out_weight.shape[0] % 64 == 0 else 1
    full_kv = (sp_count * rows, keys.shape[1])
    hbm = pl.BlockSpec(memory_space=pl.ANY)
    return pl.pallas_call(
        functools.partial(attention_kernel, planes, lanes_x, outer_dp, inner_dp),
        name="gathered_attention",
        out_shape=(
            jax.ShapeDtypeStruct((rows, width), jnp.bfloat16),
            jax.ShapeDtypeStruct((rows, width), jnp.bfloat16),
        ),
        in_specs=[hbm, vmem, hbm] + [vmem] * 4 + [hbm, vmem, hbm],
        out_specs=(vmem, vmem),
        scratch_shapes=[
            pltpu.VMEM(query.shape, jnp.bfloat16),
            pltpu.VMEM(resid.shape, jnp.bfloat16),
            pltpu.VMEM(full_kv, jnp.bfloat16),
            pltpu.VMEM(full_kv, jnp.bfloat16),
            pltpu.VMEM((dp_count * out_weight.shape[0], width), jnp.bfloat16),
            pltpu.VMEM((q_heads, rows, head_dim), jnp.bfloat16),
            pltpu.VMEM((q_heads, rows, head_dim), jnp.float32),
            pltpu.VMEM((q_heads, rows, head_dim), jnp.float32),
            pltpu.VMEM((q_heads, rows, head_dim), jnp.float32),
            pltpu.VMEM((rows, q_heads * head_dim), jnp.bfloat16),
            dma((lanes_x,)), dma((lanes_x,)),
            dma((hops * lanes_x,)), dma((hops * lanes_x,)),
            dma((hops,)), dma((hops,)),
            dma(((hops + 1) * lanes_x,)), dma(((hops + 1) * lanes_x,)),
            dma((hops,)), dma((hops,)),
            dma(((hops + 1) * lanes_x,)), dma(((hops + 1) * lanes_x,)),
            dma((outer_dp * pieces,)), dma((outer_dp * pieces,)),
            dma((outer_dp * inner_dp * pieces,)), dma((outer_dp * inner_dp * pieces,)),
            dma((4,)),
        ],
        compiler_params=pltpu.CompilerParams(
            collective_id=0, has_side_effects=True, vmem_limit_bytes=VMEM_BYTES
        ),
    )(
        query, keys, values, q_gain[None], k_gain[None], cosine, sine, resid,
        norm_gain[None], out_weight,
    )


def experts_kernel(
    planes, lanes_x, slots,
    ids_ref, scale_ref, normed_ref, upd_hbm, gate_hbm, up_hbm, down_hbm,
    out_ref,
    meta, upd_ref, raw, pk, epk, xb, rb, fr, fp, ptab, whi, wlo, tri, xs, sums, act, acc, gate_w, up_w, down_w,
    meta_s, meta_r, zs, zr, es, er, rs, rr, fs, fa, loc,
):
    Z, X, K = planes, lanes_x, slots
    rows, width = normed_ref.shape
    DP = lax.axis_size("dp")
    EP = X * DP
    S = EP * K
    top = ids_ref.shape[0]
    chunks = zr.shape[1]
    part = width // chunks
    hidden = gate_w.shape[1]
    sp, dp = lax.axis_index("sp"), lax.axis_index("dp")
    z, x = sp // X, sp % X
    p = x * DP + dp
    f32, bf16 = jnp.float32, jnp.bfloat16

    def cols(ck):
        return pl.ds(pl.multiple_of(ck * part, part), part)

    def peer(q):
        return (z * X + q // DP, q % DP)

    def loop(low, high, body):
        def step(i, carry):
            body(i)
            return carry
        lax.fori_loop(low, high, step, 0)

    def remote(src, dst, ssem, rsem, device):
        return pltpu.make_async_remote_copy(
            src_ref=src, dst_ref=dst, send_sem=ssem, recv_sem=rsem,
            device_id=device, device_id_type=MESH,
        )

    weights = [
        pltpu.make_async_copy(gate_hbm, gate_w, loc.at[0]),
        pltpu.make_async_copy(up_hbm, up_w, loc.at[1]),
        pltpu.make_async_copy(down_hbm, down_w, loc.at[2]),
    ]

    barrier = pltpu.get_barrier_semaphore()

    def greet(device):
        pl.semaphore_signal(barrier, inc=1, device_id=device, device_id_type=MESH)

    loop(1, EP, lambda j: greet(peer((p + j) % EP)))
    for j in range(1, Z):
        greet((((z + j) % Z) * X + x, dp))
    for copy in weights:
        copy.start()
    upd_copy = pltpu.make_async_copy(upd_hbm, upd_ref, loc.at[3])
    upd_copy.start()
    meta[z, :top] = ids_ref[...].astype(f32)
    meta[z, top:] = scale_ref[...]
    tri[...] = (
        lax.broadcasted_iota(jnp.int32, (rows, rows), 0)
        < lax.broadcasted_iota(jnp.int32, (rows, rows), 1)
    ).astype(f32).astype(bf16)
    pl.semaphore_wait(barrier, EP - 1 + Z - 1)

    def toward(d):
        return 1 - 2 * d

    def side(d):
        return (sp + X * toward(d), dp)

    def end_of(d):
        return (Z - 1) * (1 - d)

    def exists(d):
        return jnp.logical_and(z + toward(d) >= 0, z + toward(d) < Z)

    def at_end(d):
        return z == end_of(d)

    def next_end(d):
        return z + toward(d) == end_of(d)

    def own_slot(d):
        return z + d * (Z - z)

    def meta_copy(j):
        return remote(
            meta.at[z], meta.at[z], meta_s.at[j], meta_r.at[z], (((z + j) % Z) * X + x, dp)
        )

    def own_raw(d, ck):
        return remote(
            normed_ref.at[:, cols(ck)], raw.at[z, :, cols(ck)],
            zs.at[own_slot(d), ck], zr.at[z, ck], side(d),
        )

    def raw_on(d, src, ck):
        return remote(
            raw.at[src, :, cols(ck)], raw.at[src, :, cols(ck)],
            zs.at[src, ck], zr.at[src, ck], side(d),
        )

    def packed_on(d, src, slot, ck):
        return remote(
            epk.at[slot, :, :, cols(ck)], pk.at[src, :, :, cols(ck)],
            zs.at[slot, ck], zr.at[src, ck], side(d),
        )

    def landed(buf, index, sem):
        view = buf.at[index]
        pltpu.make_async_copy(view, view, sem).wait()

    def spread(src, ck):
        pltpu.make_async_copy(
            pk.at[src, p, :, cols(ck)], xb.at[src, p, :, cols(ck)], er.at[src, ck]
        ).start()

        def one(j):
            q = (p + j) % EP
            remote(
                pk.at[src, q, :, cols(ck)], xb.at[src, p, :, cols(ck)],
                es.at[src, ck], er.at[src, ck], peer(q),
            ).start()

        loop(1, EP, one)

    def give_back(src, ck):
        pltpu.make_async_copy(
            xb.at[src, p, :, cols(ck)], rb.at[src, p, :, cols(ck)], rr.at[src, ck]
        ).start()

        def one(j):
            q = (p + j) % EP
            remote(
                xb.at[src, q, :, cols(ck)], rb.at[src, p, :, cols(ck)],
                rs.at[src, ck], rr.at[src, ck], peer(q),
            ).start()

        loop(1, EP, one)

    def build(src, plane, index):
        info = meta[src]
        lane_expert = (
            lax.broadcasted_iota(jnp.int32, (EP, rows), 0) + plane * EP
        ).astype(f32)
        named = jnp.zeros((EP, rows), f32)
        scale = jnp.zeros((EP, rows), f32)
        for i in range(top):
            hit = info[i:i + 1] == lane_expert
            named = jnp.where(hit, 1.0, named)
            scale = jnp.where(hit, info[top + i:top + i + 1], scale)
        rank = jnp.dot(named.astype(bf16), tri[...], preferred_element_type=f32)
        rank = jnp.where(named > 0.0, rank, -1.0)
        place = lax.broadcasted_iota(jnp.int32, (K, rows), 0).astype(f32)
        ones, scaled = [], []
        for e in range(EP):
            one = jnp.where(rank[e:e + 1] == place, 1.0, 0.0)
            ones.append(one)
            scaled.append(one * scale[e:e + 1])
        ptab[index] = jnp.concatenate(ones, axis=0).astype(bf16)
        spare = whi.shape[2] - S
        if spare:
            scaled.append(jnp.zeros((spare, rows), f32))
        turned = jnp.concatenate(scaled, axis=0).T
        high = turned.astype(bf16)
        whi[index] = high
        wlo[index] = (turned - high.astype(f32)).astype(bf16)

    def pack(index, value):
        got = jnp.dot(ptab[index], value, preferred_element_type=f32)
        return got.reshape(EP, K, part).astype(bf16)

    def unpack(index, value):
        flat = value.reshape(S, part)
        return jnp.dot(whi[index, :, :S], flat, preferred_element_type=f32) + jnp.dot(
            wlo[index, :, :S], flat, preferred_element_type=f32
        )

    for j in range(1, Z):
        meta_copy(j).start()

    def own_raw_start(d):
        @pl.when(jnp.logical_and(exists(d), jnp.logical_not(next_end(d))))
        def _():
            loop(0, chunks, lambda ck: own_raw(d, ck).start())

    loop(0, 2, own_raw_start)

    def own_packed(d, low, high):
        @pl.when(jnp.logical_and(exists(d), next_end(d)))
        def _():
            slot = own_slot(d)

            def chunk(ck):
                epk[slot, :, :, cols(ck)] = pack(Z + slot, normed_ref[:, cols(ck)])
                packed_on(d, z, slot, ck).start()

            loop(low, high, chunk)

    def own_packed_start(d):
        @pl.when(jnp.logical_and(exists(d), next_end(d)))
        def _():
            build(z, end_of(d), Z + own_slot(d))

        own_packed(d, 0, early)

    early = -(-chunks // 2)
    last = chunks - 1
    is_end = jnp.logical_or(z == 0, z == Z - 1)
    loop(0, 2, own_packed_start)
    build(z, z, z)

    def own_chunk(ck):
        pk[z, :, :, cols(ck)] = pack(z, normed_ref[:, cols(ck)])
        spread(z, ck)

    loop(0, chunks, own_chunk)

    def held(src, ck):
        near = jnp.logical_or(src == z + 1, src == z - 1)
        return jnp.logical_and(near, ck >= early) if Z > 2 else False

    def carry_on(d, src, ck):
        @pl.when(ck == 0)
        def _():
            pltpu.make_async_copy(meta.at[src], meta.at[src], meta_r.at[src]).wait()

        @pl.when(at_end(d))
        def _():
            @pl.when(jnp.logical_not(held(src, ck)))
            def _():
                landed(pk, (src, slice(None), slice(None), cols(ck)), zr.at[src, ck])
                spread(src, ck)

        @pl.when(jnp.logical_not(at_end(d)))
        def _():
            @pl.when(ck == 0)
            def _():
                build(src, z, src)

                @pl.when(next_end(d))
                def _():
                    build(src, end_of(d), Z + src)

            landed(raw, (src, slice(None), cols(ck)), zr.at[src, ck])

            @pl.when(jnp.logical_not(next_end(d)))
            def _():
                raw_on(d, src, ck).start()

            @pl.when(next_end(d))
            def _():
                epk[src, :, :, cols(ck)] = pack(Z + src, raw[src, :, cols(ck)])
                packed_on(d, src, src, ck).start()

            pk[src, :, :, cols(ck)] = pack(src, raw[src, :, cols(ck)])
            spread(src, ck)

    tile = min(256, hidden)

    def run_expert(src, now):
        def gather(ck):
            landed(xb, (src, slice(None), slice(None), cols(ck)), er.at[src, ck])
            xs[:, cols(ck)] = xb[src, :, :, cols(ck)].reshape(S, part)

        def products(at, low, high):
            span = slice(low * part, high * part)
            return [
                jnp.dot(xs[:, span], matrix[span, at], preferred_element_type=f32)
                for matrix in (gate_w, up_w)
            ]

        def spot(n):
            return pl.ds(pl.multiple_of(n * tile, tile), tile)

        def begin(n):
            for i, value in enumerate(products(spot(n), 0, chunks - 1)):
                sums[i, :, spot(n)] = value

        def inner(n):
            values = products(spot(n), chunks - 1 if chunks > 1 else 0, chunks)
            if chunks > 1:
                values = [value + sums[i, :, spot(n)] for i, value in enumerate(values)]
            gated = jnp.minimum(values[0], LIMIT)
            linear = jnp.clip(values[1], -LIMIT, LIMIT)
            act[:, spot(n)] = (
                gated * jax.nn.sigmoid(SLOPE * gated) * (linear + 1.0)
            ).astype(bf16)

        if chunks > 1:
            loop(0, chunks - 1, gather)
            loop(0, hidden // tile, begin)
        gather(chunks - 1)
        loop(0, hidden // tile, inner)

        def outer(ck):
            result = jnp.dot(act[...], down_w[:, cols(ck)], preferred_element_type=f32)
            xb[src, :, :, cols(ck)] = result.reshape(EP, K, part).astype(bf16)

            if now:
                give_back(src, ck)

        loop(0, chunks, outer)

    def far_slot(d, src):
        return jnp.where(jnp.logical_and(d == 1, z + 1 == src), Z, src)

    def back_packed(d, src, ck):
        return remote(
            rb.at[src, :, :, cols(ck)], fp.at[far_slot(d, src), :, :, cols(ck)],
            fs.at[src, ck], fa.at[far_slot(d, src), ck], side(1 - d),
        )

    def back_raw(d, src, ck):
        return remote(
            raw.at[src, :, cols(ck)], fr.at[far_slot(d, src), :, cols(ck)],
            fs.at[src, ck], fa.at[far_slot(d, src), ck], side(1 - d),
        )

    def add_far(d, slot, ck):
        @pl.when(next_end(d))
        def _():
            landed(fp, (slot, slice(None), slice(None), cols(ck)), fa.at[slot, ck])
            acc[...] += unpack(Z + slot, fp[slot, :, :, cols(ck)])

        @pl.when(jnp.logical_not(next_end(d)))
        def _():
            landed(fr, (slot, slice(None), cols(ck)), fa.at[slot, ck])
            acc[...] += fr[slot, :, cols(ck)].astype(f32)

    def returned(src, ck):
        landed(rb, (src, slice(None), slice(None), cols(ck)), rr.at[src, ck])

    def send_back(d, src, ck):
        returned(src, ck)

        @pl.when(at_end(d))
        def _():
            back_packed(d, src, ck).start()

        @pl.when(jnp.logical_not(at_end(d)))
        def _():
            acc[...] = unpack(src, rb[src, :, :, cols(ck)])
            add_far(d, src, ck)

            @pl.when(jnp.logical_not(next_end(d)))
            def _():
                raw_on(d, src, ck).wait_send()

            raw[src, :, cols(ck)] = acc[...].astype(bf16)
            back_raw(d, src, ck).start()

    def wait_weights():
        for copy in weights:
            copy.wait()

    def backward(k, low, high):
        def turn(i):
            def one(t):
                d, ck = inward(t), i - t
                src = (Z - 1 - k) * (1 - d) + k * d
                ready = jnp.logical_and(ck >= low, ck < high)

                @pl.when(jnp.logical_and(ready, (z - src) * toward(d) > 0))
                def _():
                    send_back(d, src, ck)

            loop(0, 2, one)

        loop(low, high + 1, turn)

    def away(s):
        if Z < 3:
            return s
        return jnp.where(jnp.logical_and(is_end, jnp.logical_and(s > 0, s < 3)), 3 - s, s)

    def inward(t):
        return jnp.where(2 * z >= Z, t, 1 - t)

    def within(src):
        return jnp.logical_and(src >= 0, src < Z)

    lead = min(2, chunks)

    def stage(s):
        def chunk(ck):
            def one(d):
                src = z - away(s) * toward(d)

                @pl.when(within(src))
                def _():
                    carry_on(d, src, ck)

            each = jnp.logical_and(is_end, jnp.logical_and(s > 2, s < Z))

            @pl.when(each)
            def _():
                backward(s - 1, ck, ck + 1)

            loop(0, 2, one)

            @pl.when(jnp.logical_and(s == 1, ck == 0))
            def _():
                wait_weights()

            def expert(far, t, now):
                src = z - far * toward(inward(t))

                @pl.when(within(src))
                def _():
                    run_expert(src, now)

            middle = jnp.logical_and(s > 1, jnp.logical_not(is_end))
            late_end = jnp.logical_and(is_end, s == 3)
            first = jnp.where(is_end, min(1, last), 0)

            before = jnp.logical_and(jnp.logical_and(s > 2, s < Z), ck == 0)

            @pl.when(jnp.logical_and(before, jnp.logical_not(is_end)))
            def _():
                backward(s - 1, 0, lead)

            @pl.when(jnp.logical_and(jnp.logical_and(s > 1, ck == first), jnp.logical_not(late_end)))
            def _():
                expert(away(s - 1), 0, True)

            @pl.when(jnp.logical_and(middle, ck == min(1, last)))
            def _():
                expert(s - 1, 1, False)

            own_turn = jnp.where(is_end, min(1, last), last)

            @pl.when(ck == last)
            def _():
                @pl.when(s == 1)
                def _():
                    loop(0, 2, lambda d: own_packed(d, early, chunks))

                if Z > 2:
                    @pl.when(jnp.logical_and(is_end, s == Z - 1))
                    def _():
                        beside = jnp.where(z == 0, 1, Z - 2)

                        def late(i):
                            landed(
                                pk, (beside, slice(None), slice(None), cols(i)), zr.at[beside, i]
                            )
                            spread(beside, i)

                        loop(early, chunks, late)

                src = z - (s - 1) * toward(inward(1))

                @pl.when(jnp.logical_and(middle, within(src)))
                def _():
                    loop(0, chunks, lambda i: give_back(src, i))

                @pl.when(s == Z)
                def _():
                    loop(0, chunks, lambda i: give_back(z, i))

            @pl.when(jnp.logical_and(s == 1, ck == own_turn))
            def _():
                run_expert(z, False)

            turn = jnp.logical_or(s == Z, jnp.logical_not(is_end))

            @pl.when(jnp.logical_and(jnp.logical_and(s > 2, ck == last), turn))
            def _():
                backward(s - 1, jnp.where(s < Z, lead, 0), chunks)

            if Z > 2:
                @pl.when(jnp.logical_and(jnp.logical_and(s == Z, ck == last), is_end))
                def _():
                    expert(away(2), 0, True)

        loop(0, chunks, chunk)

    loop(1, Z + 1, stage)
    if Z > 1:
        backward(1, 0, chunks)

    upd_copy.wait()

    def finish(ck):
        returned(z, ck)
        acc[...] = upd_ref[:, cols(ck)].astype(f32) + unpack(z, rb[z, :, :, cols(ck)])

        def beyond(d):
            @pl.when(exists(d))
            def _():
                add_far(d, own_slot(d), ck)

        loop(0, 2, beyond)
        out_ref[:, cols(ck)] = acc[...].astype(bf16)

    loop(0, chunks, finish)

    for j in range(1, Z):
        meta_copy(j).wait_send()

    def sent_all(ck):
        def own_sent(d):
            @pl.when(jnp.logical_and(exists(d), jnp.logical_not(next_end(d))))
            def _():
                own_raw(d, ck).wait_send()

            @pl.when(jnp.logical_and(exists(d), next_end(d)))
            def _():
                packed_on(d, z, own_slot(d), ck).wait_send()

        loop(0, 2, own_sent)

        def per_source(src):
            some = pl.ds(0, EP - 1)
            landed(pk, (src, some, slice(None), cols(ck)), es.at[src, ck])
            landed(xb, (src, some, slice(None), cols(ck)), rs.at[src, ck])
            d = jnp.where(src < z, 0, 1)

            @pl.when(src != z)
            def _():
                @pl.when(at_end(d))
                def _():
                    back_packed(d, src, ck).wait_send()

                @pl.when(jnp.logical_not(at_end(d)))
                def _():
                    back_raw(d, src, ck).wait_send()

                    @pl.when(next_end(d))
                    def _():
                        packed_on(d, src, src, ck).wait_send()

        loop(0, Z, per_source)

    loop(0, chunks, sent_all)


def experts(route_ids, route_weight, normed, updated, gate_matrix, up_matrix, down_matrix):
    sp_count, dp_count = lax.axis_size("sp"), lax.axis_size("dp")
    planes = 4 if sp_count % 4 == 0 else 1
    lanes_x = sp_count // planes
    rows, width = normed.shape
    top = route_ids.shape[1]
    capacity = max(2, 3 * rows * top // (2 * sp_count * dp_count))
    slots = -(-capacity // 8) * 8
    group = lanes_x * dp_count
    padded = -(-group * slots // 128) * 128
    hidden = gate_matrix.shape[1]
    chunks = CHUNKS if width % (128 * CHUNKS) == 0 else 1
    dma = pltpu.SemaphoreType.DMA
    vmem = pl.BlockSpec(memory_space=pltpu.VMEM)
    hbm = pl.BlockSpec(memory_space=pl.ANY)
    bf16, f32 = jnp.bfloat16, jnp.float32
    return pl.pallas_call(
        functools.partial(experts_kernel, planes, lanes_x, slots),
        name="routed_experts",
        out_shape=jax.ShapeDtypeStruct((rows, width), bf16),
        in_specs=[vmem] * 3 + [hbm] * 4,
        out_specs=vmem,
        scratch_shapes=[
            pltpu.VMEM((planes, 2 * top, rows), f32),
            pltpu.VMEM((rows, width), bf16),
            pltpu.VMEM((planes, rows, width), bf16),
            pltpu.VMEM((planes, group, slots, width), bf16),
            pltpu.VMEM((planes + 1, group, slots, width), bf16),
            pltpu.VMEM((planes, group, slots, width), bf16),
            pltpu.VMEM((planes, group, slots, width), bf16),
            pltpu.VMEM((planes + 1, rows, width), bf16),
            pltpu.VMEM((planes + 1, group, slots, width), bf16),
            pltpu.VMEM((2 * planes + 1, group * slots, rows), bf16),
            pltpu.VMEM((2 * planes + 1, rows, padded), bf16),
            pltpu.VMEM((2 * planes + 1, rows, padded), bf16),
            pltpu.VMEM((rows, rows), bf16),
            pltpu.VMEM((group * slots, width), bf16),
            pltpu.VMEM((2, group * slots, hidden), f32),
            pltpu.VMEM((group * slots, hidden), bf16),
            pltpu.VMEM((rows, width // chunks), f32),
            pltpu.VMEM(gate_matrix.shape, bf16),
            pltpu.VMEM(up_matrix.shape, bf16),
            pltpu.VMEM(down_matrix.shape, bf16),
            dma((planes,)), dma((planes,)),
            dma((planes + 1, chunks)), dma((planes, chunks)),
            dma((planes, chunks)), dma((planes, chunks)),
            dma((planes, chunks)), dma((planes, chunks)),
            dma((planes, chunks)), dma((planes + 1, chunks)),
            dma((4,)),
        ],
        compiler_params=pltpu.CompilerParams(
            collective_id=1, has_side_effects=True, vmem_limit_bytes=VMEM_BYTES
        ),
    )(route_ids.T, route_weight.T, normed, updated, gate_matrix, up_matrix, down_matrix)


def per_device(
    resid,
    query,
    keys,
    values,
    q_gain,
    k_gain,
    out_weight,
    norm_gain,
    route_ids,
    route_weight,
    expert_gate,
    expert_up,
    expert_down,
):
    tok_rows = resid.shape[1]
    head_dim = q_gain.shape[0]
    places = lax.axis_index("sp") * tok_rows + jnp.arange(tok_rows, dtype=jnp.int32)
    cosine, sine = turn_tables(places, head_dim)
    updated, normed = attention(
        query[0], keys[0], values[0], q_gain, k_gain, cosine, sine, resid[0], norm_gain, out_weight
    )
    return experts(
        route_ids[0], route_weight[0], normed, updated,
        expert_gate[0], expert_up[0], expert_down[0],
    )[None]


def solution(mesh):
    placed = (
        P("dp", "sp", None),
        P("dp", "sp", None),
        P("dp", "sp", None),
        P("dp", "sp", None),
        P(),
        P(),
        P("dp", None),
        P(),
        P("dp", "sp", None),
        P("dp", "sp", None),
        P(("sp", "dp"), None, None),
        P(("sp", "dp"), None, None),
        P(("sp", "dp"), None, None),
    )
    return jax.shard_map(
        per_device, mesh=mesh, in_specs=placed, out_specs=P("dp", "sp", None), check_vma=False
    )
```
